256 devices in a mesh: grp: 2 (over y), row: 16 (over z), col: 8 (over x, core).
Axes of the slice: x: 4, y: 2, z: 16, core: 2. Of those that a mesh axis runs over, the one named last changes fastest.
The devices are a block of a 4x16x16 slice.
Arguments:
- tokens: bfloat16 [8192, 2048], P(('grp', 'row')), parts along dimension 0, may hold values from -6 to 6
- w_value: bfloat16 [2048, 2048], P(None, 'col'), may hold values from -0.125 to 0.125
- w_gate_a: bfloat16 [2048, 2048], P(None, 'col'), may hold values from -0.125 to 0.125
- w_gate_b: bfloat16 [2048, 2048], P(None, 'col'), may hold values from -0.125 to 0.125
- short_taps: bfloat16 [3, 3, 2048], replicated, may hold values from -3.5 to 3.5
- pos_weight: float32 [33, 64], replicated, may hold values from -3 to 3
- pos_bias: float32 [64], replicated, may hold values from -3 to 3
- sine_freq: float32 [2, 64], replicated, may hold values from 1.2 to 2
- hid_weight: float32 [64, 64], replicated, may hold values from -1.5 to 1.5
- hid_bias: float32 [64], replicated, may hold values from -3 to 3
- filter_out: float32 [64, 2, 2, 2048], P(None, None, None, 'col'), may hold values from -0.0234375 to 0.0234375
- filter_bias: float32 [2, 2048], replicated, may hold values from -3 to 3
- lag_decay: float32 [2048], replicated, may hold values from 1 to 137, as said below
Outputs:
- mixed: bfloat16 [8192, 2048], P(('grp', 'row'), 'col'), parts along dimension 0
The draws below stay inside these ranges and needn't reach their ends.
There are 2 independent parts, one for each index of `grp`. The reference program is written for one: setup_inputs(seed, part) draws one part's arguments, and reference() takes and returns one part's arrays. A program takes and returns all parts, laid end to end along the dimension named above; an argument that names none is the same for every part. Nothing has to cross between parts.
Inputs may be any that keep to these rules, and one draw needn't show every extreme that they name: `lag_decay`: each channel's envelope decay is positive.
All inputs are finite; a program needn't handle non-finite values.
Results may differ from the reference program's by a relative error of at most 0.0081.
Values may be sent and summed in bfloat16 or wider, within the bound.
A program may use at most 64 MiB of HBM per device.

```python
import math
import jax
import jax.numpy as jnp
from jax import lax

D = 2048
HID = 64
PE = 33
SEQ = 4096


def draw_lag_decay(key, part):
    pick_key = jax.random.fold_in(key, 11)
    slow_key = jax.random.fold_in(key, 12)
    fast_key = jax.random.fold_in(key, 13)
    slow_rates = jnp.exp(jax.random.uniform(slow_key, (D,), jnp.float32, 0.0, math.log(2.3)))
    fast_low = max(SEQ / 100.0, 3.0)
    fast_high = max(SEQ / 30.0, 6.0)
    fast_rates = jnp.exp(jax.random.uniform(fast_key, (D,), jnp.float32, math.log(fast_low), math.log(fast_high)))
    fast_share = 0.5
    chosen = jax.random.bernoulli(pick_key, fast_share, (D,))
    return jnp.where(chosen, fast_rates, slow_rates).astype(jnp.float32)


def shard_levels(own_key, dims, split, smallest, top_value):
    def one(axis_at, parts):
        heights = jax.random.uniform(jax.random.fold_in(jax.random.fold_in(own_key, 6), axis_at), (parts,), jnp.float32, smallest / len(split), top_value / len(split))
        return jnp.repeat(jnp.exp(heights), dims[axis_at] // parts).reshape((-1,) + (1,) * (len(dims) - axis_at - 1))

    level = one(*split[0])
    for cut in split[1:]:
        level = level * one(*cut)
    return level


def centred(key, shape, spread, most, cuts=(), kind=jnp.bfloat16):
    loudness = shard_levels(key, shape, cuts, -0.22, 0.18) if cuts else 1.0
    entries = jax.random.normal(key, shape, jnp.float32) * spread * loudness
    return jnp.minimum(jnp.maximum(entries, -most), most).astype(kind)


def setup_inputs(seed: int = 0, part: int = 0) -> dict:
    key_of = jax.random.split(jax.random.key(seed), 14)
    part_keys = jax.random.split(jax.random.fold_in(key_of[13], part), 14)
    tokens = centred(part_keys[0], (SEQ, D), 1.0, 6.0, ((0, 16),))
    w_value = centred(key_of[1], (D, D), D ** -0.5, 0.125, ((1, 8),))
    w_gate_a = centred(key_of[2], (D, D), D ** -0.5, 0.125, ((1, 8),))
    w_gate_b = centred(key_of[3], (D, D), D ** -0.5, 0.125, ((1, 8),))
    short_taps = centred(key_of[4], (3, 3, D), 3 ** -0.5, 3.5)
    pos_weight = centred(key_of[5], (PE, HID), 1.0, 3.0, (), jnp.float32)
    pos_bias = centred(key_of[6], (HID,), 0.5, 3.0, (), jnp.float32)
    sine_freq = jnp.clip(jax.random.uniform(key_of[7], (2, HID), jnp.float32, 1.2, 2.0), 1.2, 2.0)
    hid_weight = centred(key_of[8], (HID, HID), 0.5, 1.5, (), jnp.float32)
    hid_bias = centred(key_of[9], (HID,), 0.5, 3.0, (), jnp.float32)
    filter_out = centred(key_of[10], (HID, 2, 2, D), (HID * SEQ // 4) ** -0.5, 0.0234375, ((3, 8),), jnp.float32)
    filter_bias = centred(key_of[11], (2, D), 0.5, 3.0, (), jnp.float32)
    lag_decay = draw_lag_decay(jax.random.fold_in(key_of[13], 71), part)
    return dict(tokens=tokens, w_value=w_value, w_gate_a=w_gate_a, w_gate_b=w_gate_b, short_taps=short_taps, pos_weight=pos_weight, pos_bias=pos_bias, sine_freq=sine_freq, hid_weight=hid_weight, hid_bias=hid_bias, filter_out=filter_out, filter_bias=filter_bias, lag_decay=lag_decay)


WINDOW_SHIFT = 0.05


def positional_features(length):
    positions = jnp.arange(length, dtype=jnp.float32)
    scaled_time = positions / max(length - 1, 1)
    band_count = (PE - 1) // 2
    frequencies = jnp.linspace(1e-4, band_count - 1, band_count, dtype=jnp.float32)
    angles = ((2.0 * math.pi / length) * positions)[:, None] * frequencies[None, :]
    features = jnp.concatenate([scaled_time[:, None], jnp.cos(angles), -jnp.sin(angles)], axis=1)
    return scaled_time, features


def short_conv(projected, tap_weights):
    widened = jnp.pad(projected.astype(jnp.float32), ((1, 1), (0, 0)))
    tap_values = tap_weights.astype(jnp.float32)
    summed = widened[:-2] * tap_values[0] + widened[1:-1] * tap_values[1] + widened[2:] * tap_values[2]
    return summed.astype(jnp.bfloat16)


def long_conv(signal, forward_part, backward_part, bias_row):
    length = signal.shape[0]
    kernel = jnp.concatenate([forward_part, jnp.zeros_like(forward_part[:1]), backward_part[:0:-1]], axis=0)
    spectrum = jnp.fft.rfft(kernel, axis=0)
    transformed = jnp.fft.rfft(signal, n=2 * length, axis=0)
    result = jnp.fft.irfft(transformed * spectrum, n=2 * length, axis=0)[:length]
    return result + signal * bias_row


def reference(tokens, w_value, w_gate_a, w_gate_b, short_taps, pos_weight, pos_bias, sine_freq, hid_weight, hid_bias, filter_out, filter_bias, lag_decay):
    projections = [jnp.dot(tokens, weight_matrix, preferred_element_type=jnp.float32).astype(jnp.bfloat16) for weight_matrix in (w_value, w_gate_a, w_gate_b)]
    value_seq = short_conv(projections[0], short_taps[0])
    gate_a_seq = short_conv(projections[1], short_taps[1])
    gate_b_seq = short_conv(projections[2], short_taps[2])
    highest = lax.Precision.HIGHEST
    scaled_time, features = positional_features(SEQ)
    hidden_a = jnp.sin(sine_freq[0] * (jnp.dot(features, pos_weight, precision=highest) + pos_bias))
    hidden_b = jnp.sin(sine_freq[1] * (jnp.dot(hidden_a, hid_weight, precision=highest) + hid_bias))
    envelope = jnp.exp(-scaled_time[:, None] * lag_decay[None, :]) + WINDOW_SHIFT

    def order_filters(order_index):
        raw_filters = jnp.dot(hidden_b, filter_out[:, order_index].reshape(HID, 2 * D), precision=highest)
        raw_filters = raw_filters.reshape(SEQ, 2, D)
        return raw_filters[:, 0] * envelope, raw_filters[:, 1] * envelope

    forward_a, backward_a = order_filters(0)
    first_conv = long_conv(value_seq.astype(jnp.float32), forward_a, backward_a, filter_bias[0])
    gated = gate_a_seq.astype(jnp.float32) * first_conv
    forward_b, backward_b = order_filters(1)
    second_conv = long_conv(gated, forward_b, backward_b, filter_bias[1])
    return (gate_b_seq.astype(jnp.float32) * second_conv).astype(jnp.bfloat16)
```

```python
import functools
import math

import jax
import jax.numpy as jnp
import numpy as np
from jax import lax
from jax.experimental import pallas as pl
from jax.experimental.pallas import tpu as pltpu
from jax.sharding import PartitionSpec as P

WINDOW_SHIFT = 0.05
MESH = pl.DeviceIdType.MESH
f32 = jnp.float32
bf16 = jnp.bfloat16
SIN_TERMS = 7


def sine_coefficients():
    nodes = 0.5 * np.cos((np.arange(400) + 0.5) * np.pi / 800)
    basis = np.polynomial.chebyshev.Chebyshev.fit(
        nodes * nodes, np.sin(2 * np.pi * nodes) / nodes, SIN_TERMS - 1, domain=[0, 0.25]
    )
    return [float(c) for c in basis.convert(kind=np.polynomial.Polynomial).coef]


def halves(values):
    high = values.astype(jnp.bfloat16)
    low = (values - high.astype(np.float32)).astype(jnp.bfloat16)
    return high, low


def make_constants(count, own, span, feature_total):
    length = count * span
    k1 = np.arange(count)[:, None] + 0.25
    outer = np.exp(2j * np.pi * k1 * np.arange(count)[None, :] / count)
    eye = np.eye(own)
    outer_rows = np.concatenate([np.kron(outer.real, eye), np.kron(outer.imag, eye)], axis=0)
    q = np.arange(span)
    inner = np.exp(2j * np.pi * (q[:, None] * q[None, :] % span) / span)
    turn = np.exp(2j * np.pi * k1 * q[None, :] / length)
    pieces = [*halves(outer_rows.astype(np.float32))]
    for part in (inner.real, inner.imag):
        pieces += [*halves(part.astype(np.float32))]
    forward = np.concatenate(pieces, axis=0)
    backward = np.concatenate([*halves(outer_rows.T.astype(np.float32))], axis=0)
    turns = np.concatenate([turn.real, turn.imag], axis=0).astype(np.float32)
    positions = np.arange(length, dtype=np.float64)
    bands = (feature_total - 1) // 2
    frequencies = np.linspace(1e-4, bands - 1, bands)
    angles = (2.0 * math.pi / length * positions)[None, :] * frequencies[:, None]
    features = np.concatenate(
        [positions[None, :] / max(length - 1, 1), np.cos(angles), -np.sin(angles)], axis=0
    )
    padded = -(-feature_total // 16) * 16
    table = np.zeros((padded, length), np.float32)
    table[:feature_total] = features
    return forward, backward, turns, np.concatenate([*halves(table)], axis=0)


def dot(a, b):
    return jnp.dot(a, b, preferred_element_type=f32)


def dot_nt(a, b):
    return lax.dot_general(a, b, (((1,), (1,)), ((), ())), preferred_element_type=f32)


def split(values):
    high = values.astype(bf16)
    return high, (values - high.astype(f32)).astype(bf16)


def pick(selector, table):
    high = table.astype(bf16)
    rest = table - high.astype(f32)
    middle = rest.astype(bf16)
    low = (rest - middle.astype(f32)).astype(bf16)
    return dot_nt(selector, high) + dot_nt(selector, middle) + dot_nt(selector, low)


def one_hot(rows, columns, first, own):
    row = lax.broadcasted_iota(jnp.int32, (rows, columns), 0)
    column = lax.broadcasted_iota(jnp.int32, (rows, columns), 1)
    return jnp.where(column == first + row % own, 1.0, 0.0).astype(bf16)


def sine_of_turns(turns, coefficients):
    u = turns - jnp.round(turns)
    square = u * u
    total = jnp.full_like(u, coefficients[-1])
    for c in coefficients[-2::-1]:
        total = total * square + c
    return total * u


def kernel(
    count,
    own,
    hid,
    coefficients,
    tokens,
    w_value,
    w_gate_a,
    w_gate_b,
    short_taps,
    pos_weight,
    pos_bias,
    sine_freq,
    hid_weight,
    hid_bias,
    filter_out,
    filter_bias,
    lag_decay,
    features,
    forward,
    backward,
    turns,
    out,
    tok_s,
    wv_s,
    wa_s,
    wb_s,
    taps_s,
    pw_s,
    pb_s,
    sf_s,
    hw_s,
    hb_s,
    fo_s,
    fb_s,
    ld_s,
    feat_s,
    fwd_s,
    bwd_s,
    turn_s,
    pw2_s,
    np_s,
    chan_s,
    send_v,
    send_a,
    send_o,
    recv_v,
    recv_a,
    recv_o,
    edge_send,
    edge_recv,
    gate_s,
    cols_s,
    kin_s,
    spec_s,
    tr_s,
    ti_s,
    local_sem,
    send_sem,
    recv_sem,
):
    me = lax.axis_index("row")
    col = lax.axis_index("col")
    span = tok_s.shape[0]
    share = wv_s.shape[1]
    length = count * span
    barrier = pltpu.get_barrier_semaphore()

    @pl.loop(1, count)
    def _(d):
        pl.semaphore_signal(
            barrier, inc=1, device_id={"row": lax.rem(me + d, count)}, device_id_type=MESH
        )

    start = pl.multiple_of(col * share, share)
    loads = [
        (tokens, tok_s),
        (w_value, wv_s),
        (w_gate_a, wa_s),
        (w_gate_b, wb_s),
        (short_taps.at[:, :, pl.ds(start, share)], taps_s),
        (pos_weight, pw_s),
        (pos_bias, pb_s),
        (sine_freq, sf_s),
        (hid_weight, hw_s),
        (hid_bias, hb_s),
        (filter_out, fo_s),
        (filter_bias.at[:, pl.ds(start, share)], fb_s),
        (lag_decay.at[:, pl.ds(start, share)], ld_s),
        (features, feat_s),
        (forward, fwd_s),
        (backward, bwd_s),
        (turns, turn_s),
    ]
    copies = [pltpu.make_async_copy(s, t, local_sem.at[i]) for i, (s, t) in enumerate(loads)]
    for c in copies:
        c.start()

    def remote(unit, d, source, target):
        to = lax.rem(me + d, count)
        return pltpu.make_async_remote_copy(
            src_ref=source.at[pl.ds(pl.multiple_of(to * own, own), own)],
            dst_ref=target.at[pl.ds(pl.multiple_of(me * own, own), own)],
            send_sem=send_sem.at[unit, d],
            recv_sem=recv_sem.at[unit, d],
            device_id={"row": to},
            device_id_type=MESH,
        )

    def exchange(unit, source, target):
        @pl.loop(0, count - 1)
        def _(i):
            far = lax.div(i + 1, 2)
            d = count // 2 + jnp.where(lax.rem(i, 2) == 1, far, -far)
            remote(unit, d, source, target).start()

        mine = pl.ds(pl.multiple_of(me * own, own), own)
        target[mine, :] = source[mine, :]

    def finish(unit, source, target):
        @pl.loop(1, count)
        def _(d):
            remote(unit, d, source, target).wait_recv()

    def finish_send(unit, source, target):
        @pl.loop(1, count)
        def _(d):
            remote(unit, d, source, target).wait_send()

    copies[0].wait()
    copies[1].wait()
    send_v[...] = dot(tok_s[...], wv_s[...]).T.astype(bf16)
    copies[2].wait()
    send_a[...] = dot(tok_s[...], wa_s[...]).T.astype(bf16)
    pl.semaphore_wait(barrier, count - 1)
    exchange(0, send_v, recv_v)
    exchange(1, send_a, recv_a)

    copies[3].wait()
    gate = dot(tok_s[...], wb_s[...]).astype(bf16).astype(f32)
    gate_s[...] = gate
    edge_send[0] = gate[span - 1 : span, :]
    edge_send[1] = gate[0:1, :]

    def edge(side):
        to = lax.rem(me + (1 if side == 0 else count - 1), count)
        return pltpu.make_async_remote_copy(
            src_ref=edge_send.at[side],
            dst_ref=edge_recv.at[side],
            send_sem=send_sem.at[3, side],
            recv_sem=recv_sem.at[3, side],
            device_id={"row": to},
            device_id_type=MESH,
        )

    edge(0).start()
    edge(1).start()

    for c in copies[4:]:
        c.wait()

    chan_s[...] = jnp.zeros_like(chan_s)
    chan_s[0:3, :] = taps_s[0].astype(f32)
    chan_s[8:11, :] = taps_s[1].astype(f32)
    chan_s[16:18, :] = fb_s[...]
    chan_s[24:25, :] = ld_s[...]
    cols_s[...] = pick(one_hot(count * own, share, me * own, own), chan_s[...])
    hid_eye = one_hot(hid, hid, 0, hid)
    feature_total = pw_s.shape[0]
    padded = feat_s.shape[0] // 2
    pw2_s[...] = jnp.zeros_like(pw2_s)
    pw2_s[0:feature_total, :] = pw_s[...]
    pw2_s[padded : padded + feature_total, :] = pw_s[...]
    np_s[...] = jnp.zeros_like(np_s)
    np_s[0:2, :] = sf_s[...]
    np_s[8:9, :] = pb_s[...]
    np_s[16:17, :] = hb_s[...]
    net = pick(hid_eye, np_s[...])
    scale_a = net[:, 0:1] * (0.5 / math.pi)
    scale_b = net[:, 1:2] * (0.5 / math.pi)
    shift_a = net[:, 8:9] * scale_a
    shift_b = net[:, 16:17] * scale_b
    first_high, first_low = split(pick(hid_eye, pw2_s[...]))
    first_low = first_low[:, :padded]

    def three(table):
        high, low = split(table)
        lane = lax.broadcasted_iota(jnp.int32, table.shape, 1)
        return jnp.where(lane < 2 * hid, high.astype(f32), low.astype(f32)).astype(bf16)

    hw = hw_s[...]
    second = three(pick(hid_eye, jnp.concatenate([hw, hw, hw], axis=0)))
    own_hot = one_hot(own, share, me * own, own)
    weights = []
    for order in range(2):
        for side in range(2):
            w = fo_s[:, order, side, :]
            weights.append(pick(own_hot, jnp.concatenate([w, w, w], axis=0)))
    third = three(jnp.concatenate(weights, axis=0))
    decay = cols_s[0:own, 24:25]

    blocks = 4
    width = length // blocks

    @pl.loop(0, blocks)
    def _(block):
        base = pl.multiple_of(block * width, width)
        feats = feat_s[:, pl.ds(base, width)]
        pre = dot(first_high, feats) + dot(first_low, feats[:padded])
        hidden = sine_of_turns(pre * scale_a + shift_a, coefficients)
        high, low = split(hidden)
        pre = dot(second, jnp.concatenate([high, low, high], axis=0))
        hidden = sine_of_turns(pre * scale_b + shift_b, coefficients)
        high, low = split(hidden)
        raw = dot(third, jnp.concatenate([high, low, high], axis=0))
        position = base + lax.broadcasted_iota(jnp.int32, (own, width), 1)
        scaled = position.astype(f32) * (1.0 / max(length - 1, 1))
        envelope = jnp.exp(-scaled * decay) + WINDOW_SHIFT
        later = jnp.where(position == 0, 0.0, envelope)
        for order in range(2):
            ahead = raw[2 * order * own : (2 * order + 1) * own] * envelope
            behind = raw[(2 * order + 1) * own : (2 * order + 2) * own] * later
            for kind, both in enumerate((ahead + behind, ahead - behind)):
                high, low = split(both)
                for part in range(width // span):
                    row = pl.multiple_of(block * (width // span) * own + part * own, own)
                    lanes = slice(part * span, (part + 1) * span)
                    kin_s[order, kind, 0, pl.ds(row, own), :] = high[:, lanes]
                    kin_s[order, kind, 1, pl.ds(row, own), :] = low[:, lanes]

    rows = count * own
    for part, target in enumerate((tr_s, ti_s)):
        one = turn_s[part * count : (part + 1) * count, :]
        target[...] = jnp.broadcast_to(one[:, None, :], (count, own, span)).reshape(rows, span)

    two = 2 * rows
    outer_high, outer_low = fwd_s.at[0:two], fwd_s.at[two : 2 * two]
    at = 2 * two
    real_high, real_low = fwd_s.at[at : at + span], fwd_s.at[at + span : at + 2 * span]
    at = at + 2 * span
    imag_high, imag_low = fwd_s.at[at : at + span], fwd_s.at[at + span : at + 2 * span]

    def by_real(a):
        return dot(a[0], real_high[...]) + dot(a[1], real_high[...]) + dot(a[0], real_low[...])

    def by_imag(a):
        return dot(a[0], imag_high[...]) + dot(a[1], imag_high[...]) + dot(a[0], imag_low[...])

    def minus(a):
        return (-a[0], -a[1])

    def outer(high, low):
        g = dot(outer_high[...], high) + dot(outer_low[...], high)
        if low is not None:
            g = g + dot(outer_high[...], low)
        real, imag = g[:rows], g[rows:]
        tr, ti = tr_s[...], ti_s[...]
        return split(real * tr - imag * ti), split(real * ti + imag * tr)

    for order in range(2):
        sr, si = outer(kin_s[order, 0, 0], kin_s[order, 0, 1])
        spec_s[order, 0] = (by_real(sr) + by_imag(minus(si))) * (1.0 / length)
        dr, di = outer(kin_s[order, 1, 0], kin_s[order, 1, 1])
        spec_s[order, 1] = (by_imag(dr) + by_real(di)) * (1.0 / length)

    def short(ref, first):
        p = ref[...].astype(f32)
        lane = lax.broadcasted_iota(jnp.int32, (rows, span), 1)
        none = jnp.zeros((own, span), f32)
        back = pltpu.roll(p, 1, 1)
        back = jnp.where(lane == 0, jnp.concatenate([none, back[:-own]], axis=0), back)
        ahead = pltpu.roll(p, span - 1, 1)
        ahead = jnp.where(lane == span - 1, jnp.concatenate([ahead[own:], none], axis=0), ahead)
        tap = [cols_s[:, first + i : first + i + 1] for i in range(3)]
        return (back * tap[0] + p * tap[1] + ahead * tap[2]).astype(bf16)

    def convolve(order, high, low, signal):
        hr, hi = outer(high, low)
        xr = by_real(hr) + by_imag(minus(hi))
        xi = by_imag(hr) + by_real(hi)
        kr, ki = spec_s[order, 0], spec_s[order, 1]
        yr = split(xr * kr - xi * ki)
        yi = split(xr * ki + xi * kr)
        ur = by_real(yr) + by_imag(yi)
        ui = by_real(yi) + by_imag(minus(yr))
        tr, ti = tr_s[...], ti_s[...]
        wr = split(ur * tr + ui * ti)
        wi = split(ui * tr - ur * ti)
        bh = bwd_s[0:rows, :]
        bl = bwd_s[rows : 2 * rows, :]
        y = dot(bh[:, :rows], wr[0]) + dot(bh[:, :rows], wr[1]) + dot(bl[:, :rows], wr[0])
        y = y + dot(bh[:, rows:], wi[0]) + dot(bh[:, rows:], wi[1]) + dot(bl[:, rows:], wi[0])
        return y + signal * cols_s[:, 16 + order : 17 + order]

    finish(0, send_v, recv_v)
    value = short(recv_v, 0)
    first_conv = convolve(0, value, None, value.astype(f32))
    finish(1, send_a, recv_a)
    gated = short(recv_a, 8).astype(f32) * first_conv
    high, low = split(gated)
    send_o[...] = convolve(1, high, low, gated).astype(bf16)
    exchange(2, send_o, recv_o)

    edge(0).wait()
    edge(1).wait()
    gate = gate_s[...]
    row = lax.broadcasted_iota(jnp.int32, (span, share), 0)
    above = jnp.where(me == 0, 0.0, edge_recv[0])
    below = jnp.where(me == count - 1, 0.0, edge_recv[1])
    back = jnp.where(row == 0, above, pltpu.roll(gate, 1, 0))
    ahead = jnp.where(row == span - 1, below, pltpu.roll(gate, span - 1, 0))
    tap = taps_s[2].astype(f32)
    gate = (back * tap[0:1] + gate * tap[1:2] + ahead * tap[2:3]).astype(bf16).astype(f32)
    finish(2, send_o, recv_o)
    out[...] = (gate * recv_o[...].astype(f32).T).astype(bf16)
    finish_send(0, send_v, recv_v)
    finish_send(1, send_a, recv_a)
    finish_send(2, send_o, recv_o)


def per_device(
    tokens,
    w_value,
    w_gate_a,
    w_gate_b,
    short_taps,
    pos_weight,
    pos_bias,
    sine_freq,
    hid_weight,
    hid_bias,
    filter_out,
    filter_bias,
    lag_decay,
):
    count = lax.axis_size("row")
    span, depth = tokens.shape
    share = w_value.shape[1]
    own = share // count
    rows = count * own
    hid = hid_weight.shape[0]
    feature_total = pos_weight.shape[0]
    forward, backward, turns, features = make_constants(count, own, span, feature_total)
    operands = [
        tokens,
        w_value,
        w_gate_a,
        w_gate_b,
        short_taps,
        pos_weight,
        pos_bias[None, :],
        sine_freq,
        hid_weight,
        hid_bias[None, :],
        filter_out,
        filter_bias,
        lag_decay[None, :],
        jnp.asarray(features),
        jnp.asarray(forward),
        jnp.asarray(backward),
        jnp.asarray(turns),
    ]
    cut = {4: (3, 3, share), 11: (2, share), 12: (1, share)}
    landing = [pltpu.VMEM(cut.get(i, x.shape), x.dtype) for i, x in enumerate(operands)]
    square = pltpu.VMEM((rows, span), bf16)
    scratch = [
        *landing,
        pltpu.VMEM((features.shape[0], hid), f32),
        pltpu.VMEM((24, hid), f32),
        pltpu.VMEM((32, share), f32),
        square,
        square,
        square,
        square,
        square,
        square,
        pltpu.VMEM((2, 1, share), f32),
        pltpu.VMEM((2, 1, share), f32),
        pltpu.VMEM((span, share), f32),
        pltpu.VMEM((rows, 32), f32),
        pltpu.VMEM((2, 2, 2, rows, span), bf16),
        pltpu.VMEM((2, 2, rows, span), f32),
        pltpu.VMEM((rows, span), f32),
        pltpu.VMEM((rows, span), f32),
        pltpu.SemaphoreType.DMA((len(operands),)),
        pltpu.SemaphoreType.DMA((4, count)),
        pltpu.SemaphoreType.DMA((4, count)),
    ]
    return pl.pallas_call(
        functools.partial(kernel, count, own, hid, sine_coefficients()),
        out_shape=jax.ShapeDtypeStruct((span, share), bf16),
        in_specs=[pl.BlockSpec(memory_space=pl.ANY)] * len(operands),
        out_specs=pl.BlockSpec(memory_space=pltpu.VMEM),
        scratch_shapes=scratch,
        compiler_params=pltpu.CompilerParams(collective_id=0, has_side_effects=True),
        name="gated_conv",
    )(*operands)


def solution(mesh):
    in_specs = (
        P(("grp", "row"), None),
        P(None, "col"),
        P(None, "col"),
        P(None, "col"),
        P(),
        P(),
        P(),
        P(),
        P(),
        P(),
        P(None, None, None, "col"),
        P(),
        P(),
    )
    out_specs = P(("grp", "row"), "col")
    return jax.shard_map(
        per_device, mesh=mesh, in_specs=in_specs, out_specs=out_specs, check_vma=False
    )
```

```python
import functools
import math

import jax
import jax.numpy as jnp
import numpy as np
from jax import lax
from jax.experimental import pallas as pl
from jax.experimental.pallas import tpu as pltpu
from jax.sharding import PartitionSpec as P

WINDOW_SHIFT = 0.05
MESH = pl.DeviceIdType.MESH
f32 = jnp.float32
bf16 = jnp.bfloat16
SIN_TERMS = 7


def sine_coefficients():
    nodes = 0.5 * np.cos((np.arange(400) + 0.5) * np.pi / 800)
    basis = np.polynomial.chebyshev.Chebyshev.fit(
        nodes * nodes, np.sin(2 * np.pi * nodes) / nodes, SIN_TERMS - 1, domain=[0, 0.25]
    )
    return [float(c) for c in basis.convert(kind=np.polynomial.Polynomial).coef]


def halves(values):
    high = values.astype(jnp.bfloat16)
    low = (values - high.astype(np.float32)).astype(jnp.bfloat16)
    return high, low


def make_constants(count, own, span, feature_total):
    length = count * span
    k1 = np.arange(count)[:, None] + 0.25
    outer = np.exp(2j * np.pi * k1 * np.arange(count)[None, :] / count)
    eye = np.eye(own)
    outer_rows = np.concatenate([np.kron(outer.real, eye), np.kron(outer.imag, eye)], axis=0)
    q = np.arange(span)
    inner = np.exp(2j * np.pi * (q[:, None] * q[None, :] % span) / span)
    turn = np.exp(2j * np.pi * k1 * q[None, :] / length)
    pieces = [*halves(outer_rows.astype(np.float32))]
    for part in (inner.real, inner.imag):
        pieces += [*halves(part.astype(np.float32))]
    forward = np.concatenate(pieces, axis=0)
    backward = np.concatenate([*halves(outer_rows.T.astype(np.float32))], axis=0)
    turns = np.concatenate([turn.real, turn.imag], axis=0).astype(np.float32)
    positions = np.arange(length, dtype=np.float64)
    bands = (feature_total - 1) // 2
    frequencies = np.linspace(1e-4, bands - 1, bands)
    angles = (2.0 * math.pi / length * positions)[None, :] * frequencies[:, None]
    features = np.concatenate(
        [positions[None, :] / max(length - 1, 1), np.cos(angles), -np.sin(angles)], axis=0
    )
    padded = -(-feature_total // 16) * 16
    table = np.zeros((padded, length), np.float32)
    table[:feature_total] = features
    return forward, backward, turns, np.concatenate([*halves(table)], axis=0)


def dot(a, b):
    return jnp.dot(a, b, preferred_element_type=f32)


def dot_nt(a, b):
    return lax.dot_general(a, b, (((1,), (1,)), ((), ())), preferred_element_type=f32)


def split(values):
    high = values.astype(bf16)
    return high, (values - high.astype(f32)).astype(bf16)


def pick(selector, table):
    high = table.astype(bf16)
    rest = table - high.astype(f32)
    middle = rest.astype(bf16)
    low = (rest - middle.astype(f32)).astype(bf16)
    return dot_nt(selector, high) + dot_nt(selector, middle) + dot_nt(selector, low)


def one_hot(rows, columns, first, own):
    row = lax.broadcasted_iota(jnp.int32, (rows, columns), 0)
    column = lax.broadcasted_iota(jnp.int32, (rows, columns), 1)
    return jnp.where(column == first + row % own, 1.0, 0.0).astype(bf16)


def sine_of_turns(turns, coefficients):
    u = turns - jnp.round(turns)
    square = u * u
    total = jnp.full_like(u, coefficients[-1])
    for c in coefficients[-2::-1]:
        total = total * square + c
    return total * u


def kernel(
    count,
    own,
    hid,
    coefficients,
    tokens,
    w_value,
    w_gate_a,
    w_gate_b,
    short_taps,
    pos_weight,
    pos_bias,
    sine_freq,
    hid_weight,
    hid_bias,
    filter_out,
    filter_bias,
    lag_decay,
    features,
    forward,
    backward,
    turns,
    out,
    tok_s,
    wv_s,
    wa_s,
    wb_s,
    taps_s,
    pw_s,
    pb_s,
    sf_s,
    hw_s,
    hb_s,
    fo_s,
    fb_s,
    ld_s,
    feat_s,
    fwd_s,
    bwd_s,
    turn_s,
    pw2_s,
    np_s,
    chan_s,
    send_v,
    send_a,
    send_o,
    recv_v,
    recv_a,
    recv_o,
    edge_send,
    edge_recv,
    gate_s,
    cols_s,
    kin_s,
    spec_s,
    tr_s,
    ti_s,
    chain_sem,
    ready_sem,
    local_sem,
    send_sem,
    recv_sem,
):
    me = lax.axis_index("row")
    col = lax.axis_index("col")
    span = tok_s.shape[0]
    share = wv_s.shape[1]
    length = count * span
    barrier = pltpu.get_barrier_semaphore()

    has_below = me > 0
    has_above = me < count - 1

    def signal(semaphore, to):
        pl.semaphore_signal(semaphore, inc=1, device_id={"row": to}, device_id_type=MESH)

    @pl.when(has_below)
    def _():
        signal(barrier, me - 1)

    @pl.when(has_above)
    def _():
        signal(barrier, me + 1)

    start = pl.multiple_of(col * share, share)
    loads = [
        (tokens, tok_s),
        (w_value, wv_s),
        (w_gate_a, wa_s),
        (w_gate_b, wb_s),
        (short_taps.at[:, :, pl.ds(start, share)], taps_s),
        (pos_weight, pw_s),
        (pos_bias, pb_s),
        (sine_freq, sf_s),
        (hid_weight, hw_s),
        (hid_bias, hb_s),
        (filter_out, fo_s),
        (filter_bias.at[:, pl.ds(start, share)], fb_s),
        (lag_decay.at[:, pl.ds(start, share)], ld_s),
        (features, feat_s),
        (forward, fwd_s),
        (backward, bwd_s),
        (turns, turn_s),
    ]
    copies = [pltpu.make_async_copy(s, t, local_sem.at[i]) for i, (s, t) in enumerate(loads)]
    for c in copies[:3]:
        c.start()

    def remote(unit, to, source, target):
        d = lax.rem(to - me + count, count)
        return pltpu.make_async_remote_copy(
            src_ref=source.at[pl.ds(pl.multiple_of(to * own, own), own)],
            dst_ref=target.at[pl.ds(pl.multiple_of(me * own, own), own)],
            send_sem=send_sem.at[unit, d],
            recv_sem=recv_sem.at[unit, d],
            device_id={"row": to},
            device_id_type=MESH,
        )

    def keep(source, target):
        mine = pl.ds(pl.multiple_of(me * own, own), own)
        target[mine, :] = source[mine, :]

    def finish(unit, source, target):
        @pl.loop(1, count)
        def _(d):
            remote(unit, lax.rem(me + d, count), source, target).wait_recv()

    def finish_send(unit, source, target):
        @pl.loop(1, count)
        def _(d):
            remote(unit, lax.rem(me + d, count), source, target).wait_send()

    copies[0].wait()
    copies[1].wait()
    for c in copies[3:]:
        c.start()
    send_v[...] = dot(tok_s[...], wv_s[...]).T.astype(bf16)
    copies[2].wait()
    send_a[...] = dot(tok_s[...], wa_s[...]).T.astype(bf16)

    pl.semaphore_wait(barrier, has_below.astype(jnp.int32) + has_above.astype(jnp.int32))

    @pl.when(me > 1)
    def _():
        pl.semaphore_wait(chain_sem, 1)

    @pl.when(jnp.logical_and(has_below, has_above))
    def _():
        signal(chain_sem, me + 1)

    @pl.loop(0, me)
    def _(to):
        signal(ready_sem.at[me], to)

    for unit, source, target in ((0, send_v, recv_v), (1, send_a, recv_a)):

        @pl.loop(0, count - 1)
        def _(i):
            far = lax.div(i + 1, 2)
            d = count // 2 + jnp.where(lax.rem(i, 2) == 1, far, -far)
            to = lax.rem(me + d, count)

            @pl.when(to < me)
            def _():
                remote(unit, to, source, target).start()

        keep(source, target)

    copies[3].wait()
    gate = dot(tok_s[...], wb_s[...]).astype(bf16).astype(f32)
    gate_s[...] = gate
    edge_send[0] = gate[span - 1 : span, :]
    edge_send[1] = gate[0:1, :]

    def edge(side):
        return pltpu.make_async_remote_copy(
            src_ref=edge_send.at[side],
            dst_ref=edge_recv.at[side],
            send_sem=send_sem.at[3, side],
            recv_sem=recv_sem.at[3, side],
            device_id={"row": me + (1 if side == 0 else -1)},
            device_id_type=MESH,
        )

    @pl.when(has_above)
    def _():
        edge(0).start()

    @pl.when(has_below)
    def _():
        edge(1).start()

    for c in copies[4:]:
        c.wait()

    chan_s[...] = jnp.zeros_like(chan_s)
    chan_s[0:3, :] = taps_s[0].astype(f32)
    chan_s[8:11, :] = taps_s[1].astype(f32)
    chan_s[16:18, :] = fb_s[...]
    chan_s[24:25, :] = ld_s[...]
    cols_s[...] = pick(one_hot(count * own, share, me * own, own), chan_s[...])
    hid_eye = one_hot(hid, hid, 0, hid)
    feature_total = pw_s.shape[0]
    padded = feat_s.shape[0] // 2
    pw2_s[...] = jnp.zeros_like(pw2_s)
    pw2_s[0:feature_total, :] = pw_s[...]
    pw2_s[padded : padded + feature_total, :] = pw_s[...]
    np_s[...] = jnp.zeros_like(np_s)
    np_s[0:2, :] = sf_s[...]
    np_s[8:9, :] = pb_s[...]
    np_s[16:17, :] = hb_s[...]
    net = pick(hid_eye, np_s[...])
    scale_a = net[:, 0:1] * (0.5 / math.pi)
    scale_b = net[:, 1:2] * (0.5 / math.pi)
    shift_a = net[:, 8:9] * scale_a
    shift_b = net[:, 16:17] * scale_b
    first_high, first_low = split(pick(hid_eye, pw2_s[...]))
    first_low = first_low[:, :padded]

    def three(table):
        high, low = split(table)
        lane = lax.broadcasted_iota(jnp.int32, table.shape, 1)
        return jnp.where(lane < 2 * hid, high.astype(f32), low.astype(f32)).astype(bf16)

    hw = hw_s[...]
    second = three(pick(hid_eye, jnp.concatenate([hw, hw, hw], axis=0)))
    own_hot = one_hot(own, share, me * own, own)
    weights = []
    for order in range(2):
        for side in range(2):
            w = fo_s[:, order, side, :]
            weights.append(pick(own_hot, jnp.concatenate([w, w, w], axis=0)))
    third = three(jnp.concatenate(weights, axis=0))
    decay = cols_s[0:own, 24:25]

    blocks = 4
    width = length // blocks

    @pl.loop(0, blocks)
    def _(block):
        base = pl.multiple_of(block * width, width)
        feats = feat_s[:, pl.ds(base, width)]
        pre = dot(first_high, feats) + dot(first_low, feats[:padded])
        hidden = sine_of_turns(pre * scale_a + shift_a, coefficients)
        high, low = split(hidden)
        pre = dot(second, jnp.concatenate([high, low, high], axis=0))
        hidden = sine_of_turns(pre * scale_b + shift_b, coefficients)
        high, low = split(hidden)
        raw = dot(third, jnp.concatenate([high, low, high], axis=0))
        position = base + lax.broadcasted_iota(jnp.int32, (own, width), 1)
        scaled = position.astype(f32) * (1.0 / max(length - 1, 1))
        envelope = jnp.exp(-scaled * decay) + WINDOW_SHIFT
        later = jnp.where(position == 0, 0.0, envelope)
        for order in range(2):
            ahead = raw[2 * order * own : (2 * order + 1) * own] * envelope
            behind = raw[(2 * order + 1) * own : (2 * order + 2) * own] * later
            for kind, both in enumerate((ahead + behind, ahead - behind)):
                high, low = split(both)
                for part in range(width // span):
                    row = pl.multiple_of(block * (width // span) * own + part * own, own)
                    lanes = slice(part * span, (part + 1) * span)
                    kin_s[order, kind, 0, pl.ds(row, own), :] = high[:, lanes]
                    kin_s[order, kind, 1, pl.ds(row, own), :] = low[:, lanes]

    rows = count * own
    for part, target in enumerate((tr_s, ti_s)):
        one = turn_s[part * count : (part + 1) * count, :]
        target[...] = jnp.broadcast_to(one[:, None, :], (count, own, span)).reshape(rows, span)

    two = 2 * rows
    outer_high, outer_low = fwd_s.at[0:two], fwd_s.at[two : 2 * two]
    at = 2 * two
    real_high, real_low = fwd_s.at[at : at + span], fwd_s.at[at + span : at + 2 * span]
    at = at + 2 * span
    imag_high, imag_low = fwd_s.at[at : at + span], fwd_s.at[at + span : at + 2 * span]

    def by_real(a):
        return dot(a[0], real_high[...]) + dot(a[1], real_high[...]) + dot(a[0], real_low[...])

    def by_imag(a):
        return dot(a[0], imag_high[...]) + dot(a[1], imag_high[...]) + dot(a[0], imag_low[...])

    def minus(a):
        return (-a[0], -a[1])

    def outer(high, low):
        g = dot(outer_high[...], high) + dot(outer_low[...], high)
        if low is not None:
            g = g + dot(outer_high[...], low)
        real, imag = g[:rows], g[rows:]
        tr, ti = tr_s[...], ti_s[...]
        return split(real * tr - imag * ti), split(real * ti + imag * tr)

    for order in range(2):
        sr, si = outer(kin_s[order, 0, 0], kin_s[order, 0, 1])
        spec_s[order, 0] = (by_real(sr) + by_imag(minus(si))) * (1.0 / length)
        dr, di = outer(kin_s[order, 1, 0], kin_s[order, 1, 1])
        spec_s[order, 1] = (by_imag(dr) + by_real(di)) * (1.0 / length)

    def short(ref, first):
        p = ref[...].astype(f32)
        lane = lax.broadcasted_iota(jnp.int32, (rows, span), 1)
        none = jnp.zeros((own, span), f32)
        back = pltpu.roll(p, 1, 1)
        back = jnp.where(lane == 0, jnp.concatenate([none, back[:-own]], axis=0), back)
        ahead = pltpu.roll(p, span - 1, 1)
        ahead = jnp.where(lane == span - 1, jnp.concatenate([ahead[own:], none], axis=0), ahead)
        tap = [cols_s[:, first + i : first + i + 1] for i in range(3)]
        return (back * tap[0] + p * tap[1] + ahead * tap[2]).astype(bf16)

    def convolve(order, high, low, signal):
        hr, hi = outer(high, low)
        xr = by_real(hr) + by_imag(minus(hi))
        xi = by_imag(hr) + by_real(hi)
        kr, ki = spec_s[order, 0], spec_s[order, 1]
        yr = split(xr * kr - xi * ki)
        yi = split(xr * ki + xi * kr)
        ur = by_real(yr) + by_imag(yi)
        ui = by_real(yi) + by_imag(minus(yr))
        tr, ti = tr_s[...], ti_s[...]
        wr = split(ur * tr + ui * ti)
        wi = split(ui * tr - ur * ti)
        bh = bwd_s[0:rows, :]
        bl = bwd_s[rows : 2 * rows, :]
        y = dot(bh[:, :rows], wr[0]) + dot(bh[:, :rows], wr[1]) + dot(bl[:, :rows], wr[0])
        y = y + dot(bh[:, rows:], wi[0]) + dot(bh[:, rows:], wi[1]) + dot(bl[:, rows:], wi[0])
        return y + signal * cols_s[:, 16 + order : 17 + order]

    @pl.loop(me + 1, count)
    def _(to):
        pl.semaphore_wait(ready_sem.at[to], 1)
        remote(0, to, send_v, recv_v).start()
        remote(1, to, send_a, recv_a).start()

    finish(0, send_v, recv_v)
    value = short(recv_v, 0)
    first_conv = convolve(0, value, None, value.astype(f32))
    finish(1, send_a, recv_a)
    gated = short(recv_a, 8).astype(f32) * first_conv
    high, low = split(gated)
    send_o[...] = convolve(1, high, low, gated).astype(bf16)

    @pl.loop(0, count)
    def _(to):
        @pl.when(to != me)
        def _():
            remote(2, to, send_o, recv_o).start()

    keep(send_o, recv_o)

    @pl.when(has_above)
    def _():
        edge(0).wait_send()
        edge(1).wait_recv()

    @pl.when(has_below)
    def _():
        edge(1).wait_send()
        edge(0).wait_recv()

    gate = gate_s[...]
    row = lax.broadcasted_iota(jnp.int32, (span, share), 0)
    above = jnp.where(me == 0, 0.0, edge_recv[0])
    below = jnp.where(me == count - 1, 0.0, edge_recv[1])
    back = jnp.where(row == 0, above, pltpu.roll(gate, 1, 0))
    ahead = jnp.where(row == span - 1, below, pltpu.roll(gate, span - 1, 0))
    tap = taps_s[2].astype(f32)
    gate = (back * tap[0:1] + gate * tap[1:2] + ahead * tap[2:3]).astype(bf16).astype(f32)
    finish(2, send_o, recv_o)
    out[...] = (gate * recv_o[...].astype(f32).T).astype(bf16)
    finish_send(0, send_v, recv_v)
    finish_send(1, send_a, recv_a)
    finish_send(2, send_o, recv_o)


def per_device(
    tokens,
    w_value,
    w_gate_a,
    w_gate_b,
    short_taps,
    pos_weight,
    pos_bias,
    sine_freq,
    hid_weight,
    hid_bias,
    filter_out,
    filter_bias,
    lag_decay,
):
    count = lax.axis_size("row")
    span, depth = tokens.shape
    share = w_value.shape[1]
    own = share // count
    rows = count * own
    hid = hid_weight.shape[0]
    feature_total = pos_weight.shape[0]
    forward, backward, turns, features = make_constants(count, own, span, feature_total)
    operands = [
        tokens,
        w_value,
        w_gate_a,
        w_gate_b,
        short_taps,
        pos_weight,
        pos_bias[None, :],
        sine_freq,
        hid_weight,
        hid_bias[None, :],
        filter_out,
        filter_bias,
        lag_decay[None, :],
        jnp.asarray(features),
        jnp.asarray(forward),
        jnp.asarray(backward),
        jnp.asarray(turns),
    ]
    cut = {4: (3, 3, share), 11: (2, share), 12: (1, share)}
    landing = [pltpu.VMEM(cut.get(i, x.shape), x.dtype) for i, x in enumerate(operands)]
    square = pltpu.VMEM((rows, span), bf16)
    scratch = [
        *landing,
        pltpu.VMEM((features.shape[0], hid), f32),
        pltpu.VMEM((24, hid), f32),
        pltpu.VMEM((32, share), f32),
        square,
        square,
        square,
        square,
        square,
        square,
        pltpu.VMEM((2, 1, share), f32),
        pltpu.VMEM((2, 1, share), f32),
        pltpu.VMEM((span, share), f32),
        pltpu.VMEM((rows, 32), f32),
        pltpu.VMEM((2, 2, 2, rows, span), bf16),
        pltpu.VMEM((2, 2, rows, span), f32),
        pltpu.VMEM((rows, span), f32),
        pltpu.VMEM((rows, span), f32),
        pltpu.SemaphoreType.REGULAR,
        pltpu.SemaphoreType.REGULAR((count,)),
        pltpu.SemaphoreType.DMA((len(operands),)),
        pltpu.SemaphoreType.DMA((4, count)),
        pltpu.SemaphoreType.DMA((4, count)),
    ]
    return pl.pallas_call(
        functools.partial(kernel, count, own, hid, sine_coefficients()),
        out_shape=pltpu.VMEM((span, share), bf16),
        in_specs=[pl.BlockSpec(memory_space=pl.ANY)] * len(operands),
        out_specs=pl.BlockSpec(memory_space=pltpu.VMEM),
        scratch_shapes=scratch,
        compiler_params=pltpu.CompilerParams(collective_id=0, has_side_effects=True),
        name="gated_conv",
    )(*operands)


def solution(mesh):
    in_specs = (
        P(("grp", "row"), None),
        P(None, "col"),
        P(None, "col"),
        P(None, "col"),
        P(),
        P(),
        P(),
        P(),
        P(),
        P(),
        P(None, None, None, "col"),
        P(),
        P(),
    )
    out_specs = P(("grp", "row"), "col")
    return jax.shard_map(
        per_device, mesh=mesh, in_specs=in_specs, out_specs=out_specs, check_vma=False
    )
```

```python
import functools
import math

import jax
import jax.numpy as jnp
import numpy as np
from jax import lax
from jax.experimental import pallas as pl
from jax.experimental.pallas import tpu as pltpu
from jax.sharding import PartitionSpec as P

WINDOW_SHIFT = 0.05
MESH = pl.DeviceIdType.MESH
f32 = jnp.float32
bf16 = jnp.bfloat16
SIN_TERMS = 7
DATA_PIECES = 2


def sine_coefficients():
    nodes = 0.5 * np.cos((np.arange(400) + 0.5) * np.pi / 800)
    basis = np.polynomial.chebyshev.Chebyshev.fit(
        nodes * nodes, np.sin(2 * np.pi * nodes) / nodes, SIN_TERMS - 1, domain=[0, 0.25]
    )
    return [float(c) for c in basis.convert(kind=np.polynomial.Polynomial).coef]


def halves(values):
    high = values.astype(jnp.bfloat16)
    low = (values - high.astype(np.float32)).astype(jnp.bfloat16)
    return high, low


def make_constants(count, own, span, feature_total):
    length = count * span
    k1 = np.arange(count)[:, None] + 0.25
    outer = np.exp(2j * np.pi * k1 * np.arange(count)[None, :] / count)
    eye = np.eye(own)
    outer_rows = np.concatenate([np.kron(outer.real, eye), np.kron(outer.imag, eye)], axis=0)
    q = np.arange(span)
    inner = np.exp(2j * np.pi * (q[:, None] * q[None, :] % span) / span)
    turn = np.exp(2j * np.pi * k1 * q[None, :] / length)
    pieces = [*halves(outer_rows.astype(np.float32))]
    for part in (inner.real, inner.imag):
        pieces += [*halves(part.astype(np.float32))]
    forward = np.concatenate(pieces, axis=0)
    backward = np.concatenate([*halves(outer_rows.T.astype(np.float32))], axis=0)
    turns = np.concatenate([turn.real, turn.imag], axis=0).astype(np.float32)
    positions = np.arange(length, dtype=np.float64)
    bands = (feature_total - 1) // 2
    frequencies = np.linspace(1e-4, bands - 1, bands)
    angles = (2.0 * math.pi / length * positions)[None, :] * frequencies[:, None]
    features = np.concatenate(
        [positions[None, :] / max(length - 1, 1), np.cos(angles), -np.sin(angles)], axis=0
    )
    padded = -(-feature_total // 16) * 16
    table = np.zeros((padded, length), np.float32)
    table[:feature_total] = features
    return forward, backward, turns, np.concatenate([*halves(table)], axis=0)


def dot(a, b):
    return jnp.dot(a, b, preferred_element_type=f32)


def dot_nt(a, b):
    return lax.dot_general(a, b, (((1,), (1,)), ((), ())), preferred_element_type=f32)


def split(values):
    high = values.astype(bf16)
    return high, (values - high.astype(f32)).astype(bf16)


def pick(selector, table):
    high = table.astype(bf16)
    rest = table - high.astype(f32)
    middle = rest.astype(bf16)
    low = (rest - middle.astype(f32)).astype(bf16)
    return dot_nt(selector, high) + dot_nt(selector, middle) + dot_nt(selector, low)


def one_hot(rows, columns, first, own):
    row = lax.broadcasted_iota(jnp.int32, (rows, columns), 0)
    column = lax.broadcasted_iota(jnp.int32, (rows, columns), 1)
    return jnp.where(column == first + row % own, 1.0, 0.0).astype(bf16)


def sine_of_turns(turns, coefficients):
    u = turns - jnp.round(turns)
    square = u * u
    total = jnp.full_like(u, coefficients[-1])
    for c in coefficients[-2::-1]:
        total = total * square + c
    return total * u


def kernel(
    count,
    own,
    hid,
    coefficients,
    tokens,
    w_value,
    w_gate_a,
    w_gate_b,
    short_taps,
    pos_weight,
    pos_bias,
    sine_freq,
    hid_weight,
    hid_bias,
    filter_out,
    filter_bias,
    lag_decay,
    features,
    forward,
    backward,
    turns,
    out,
    tok_s,
    wv_s,
    wa_s,
    wb_s,
    taps_s,
    pw_s,
    pb_s,
    sf_s,
    hw_s,
    hb_s,
    fo_s,
    fb_s,
    ld_s,
    feat_s,
    fwd_s,
    bwd_s,
    turn_s,
    pw2_s,
    np_s,
    chan_s,
    send_va,
    recv_va,
    send_o,
    recv_o,
    edge_send,
    edge_recv,
    gate_s,
    cols_s,
    kin_s,
    spec_s,
    tr_s,
    ti_s,
    ready_sem,
    local_sem,
    send_sem,
    recv_sem,
):
    me = lax.axis_index("row")
    col = lax.axis_index("col")
    span = tok_s.shape[0]
    share = wv_s.shape[1]
    length = count * span
    barrier = pltpu.get_barrier_semaphore()

    has_below = me > 0
    has_above = me < count - 1
    rank = lax.rem(me + count - 1, count)

    def signal(semaphore, to):
        pl.semaphore_signal(semaphore, inc=1, device_id={"row": to}, device_id_type=MESH)

    start = pl.multiple_of(col * share, share)
    loads = [
        (tokens, tok_s),
        (w_value, wv_s),
        (w_gate_a, wa_s),
        (w_gate_b, wb_s),
        (short_taps.at[:, :, pl.ds(start, share)], taps_s),
        (pos_weight, pw_s),
        (pos_bias, pb_s),
        (sine_freq, sf_s),
        (hid_weight, hw_s),
        (hid_bias, hb_s),
        (filter_out, fo_s),
        (filter_bias.at[:, pl.ds(start, share)], fb_s),
        (lag_decay.at[:, pl.ds(start, share)], ld_s),
        (features, feat_s),
        (forward, fwd_s),
        (backward, bwd_s),
        (turns, turn_s),
    ]
    copies = [pltpu.make_async_copy(s, t, local_sem.at[i]) for i, (s, t) in enumerate(loads)]
    for c in copies[:3]:
        c.start()

    @pl.loop(rank + 1, count)
    def _(other):
        signal(barrier, lax.rem(other + 1, count))

    @pl.when(rank > 0)
    def _():
        pl.semaphore_wait(barrier, rank)

    @pl.loop(0, rank)
    def _(other):
        signal(ready_sem.at[me], lax.rem(other + 1, count))

    def remote_pair(to):
        d = lax.rem(to - me + count, count)
        return pltpu.make_async_remote_copy(
            src_ref=send_va.at[to],
            dst_ref=recv_va.at[me],
            send_sem=send_sem.at[0, d],
            recv_sem=recv_sem.at[0, d],
            device_id={"row": to},
            device_id_type=MESH,
        )

    def remote(unit, to, source, target):
        d = lax.rem(to - me + count, count)
        return pltpu.make_async_remote_copy(
            src_ref=source.at[pl.ds(pl.multiple_of(to * own, own), own)],
            dst_ref=target.at[pl.ds(pl.multiple_of(me * own, own), own)],
            send_sem=send_sem.at[unit, d],
            recv_sem=recv_sem.at[unit, d],
            device_id={"row": to},
            device_id_type=MESH,
        )

    def to_all(body):
        @pl.loop(1, count)
        def _(d):
            body(lax.rem(me + d, count))

    copies[0].wait()
    copies[1].wait()
    for c in copies[3:]:
        c.start()
    send_va[:, 0] = dot(tok_s[...], wv_s[...]).T.astype(bf16).reshape(count, own, span)
    copies[2].wait()
    send_va[:, 1] = dot(tok_s[...], wa_s[...]).T.astype(bf16).reshape(count, own, span)

    @pl.loop(0, count - 1)
    def _(i):
        d = lax.div(i, 2) + 1
        to = lax.rem(me + jnp.where(lax.rem(i, 2) == 0, d, count - d), count)

        @pl.when(lax.rem(to + count - 1, count) < rank)
        def _():
            remote_pair(to).start()

    recv_va[me] = send_va[me]

    copies[3].wait()
    gate = dot(tok_s[...], wb_s[...]).astype(bf16).astype(f32)
    gate_s[...] = gate
    edge_send[0] = gate[span - 1 : span, :]
    edge_send[1] = gate[0:1, :]

    def edge(side):
        return pltpu.make_async_remote_copy(
            src_ref=edge_send.at[side],
            dst_ref=edge_recv.at[side],
            send_sem=send_sem.at[2, side],
            recv_sem=recv_sem.at[2, side],
            device_id={"row": me + (1 if side == 0 else -1)},
            device_id_type=MESH,
        )

    for c in copies[4:]:
        c.wait()

    chan_s[...] = jnp.zeros_like(chan_s)
    chan_s[0:3, :] = taps_s[0].astype(f32)
    chan_s[8:11, :] = taps_s[1].astype(f32)
    chan_s[16:18, :] = fb_s[...]
    chan_s[24:25, :] = ld_s[...]
    cols_s[...] = pick(one_hot(count * own, share, me * own, own), chan_s[...])
    hid_eye = one_hot(hid, hid, 0, hid)
    feature_total = pw_s.shape[0]
    padded = feat_s.shape[0] // 2
    pw2_s[...] = jnp.zeros_like(pw2_s)
    pw2_s[0:feature_total, :] = pw_s[...]
    pw2_s[padded : padded + feature_total, :] = pw_s[...]
    np_s[...] = jnp.zeros_like(np_s)
    np_s[0:2, :] = sf_s[...]
    np_s[8:9, :] = pb_s[...]
    np_s[16:17, :] = hb_s[...]
    net = pick(hid_eye, np_s[...])
    scale_a = net[:, 0:1] * (0.5 / math.pi)
    scale_b = net[:, 1:2] * (0.5 / math.pi)
    shift_a = net[:, 8:9] * scale_a
    shift_b = net[:, 16:17] * scale_b
    first_high, first_low = split(pick(hid_eye, pw2_s[...]))
    first_low = first_low[:, :padded]

    def three(table):
        high, low = split(table)
        lane = lax.broadcasted_iota(jnp.int32, table.shape, 1)
        return jnp.where(lane < 2 * hid, high.astype(f32), low.astype(f32)).astype(bf16)

    hw = hw_s[...]
    second = three(pick(hid_eye, jnp.concatenate([hw, hw, hw], axis=0)))
    own_hot = one_hot(own, share, me * own, own)
    weights = []
    for order in range(2):
        for side in range(2):
            w = fo_s[:, order, side, :]
            weights.append(pick(own_hot, jnp.concatenate([w, w, w], axis=0)))
    third = three(jnp.concatenate(weights, axis=0))
    decay = cols_s[0:own, 24:25]

    blocks = 4
    width = length // blocks

    @pl.loop(0, blocks)
    def _(block):
        base = pl.multiple_of(block * width, width)
        feats = feat_s[:, pl.ds(base, width)]
        pre = dot(first_high, feats) + dot(first_low, feats[:padded])
        hidden = sine_of_turns(pre * scale_a + shift_a, coefficients)
        high, low = split(hidden)
        pre = dot(second, jnp.concatenate([high, low, high], axis=0))
        hidden = sine_of_turns(pre * scale_b + shift_b, coefficients)
        high, low = split(hidden)
        raw = dot(third, jnp.concatenate([high, low, high], axis=0))
        position = base + lax.broadcasted_iota(jnp.int32, (own, width), 1)
        scaled = position.astype(f32) * (1.0 / max(length - 1, 1))
        envelope = jnp.exp(-scaled * decay) + WINDOW_SHIFT
        later = jnp.where(position == 0, 0.0, envelope)
        for order in range(2):
            ahead = raw[2 * order * own : (2 * order + 1) * own] * envelope
            behind = raw[(2 * order + 1) * own : (2 * order + 2) * own] * later
            for kind, both in enumerate((ahead + behind, ahead - behind)):
                high, low = split(both)
                for part in range(width // span):
                    row = pl.multiple_of(block * (width // span) * own + part * own, own)
                    lanes = slice(part * span, (part + 1) * span)
                    kin_s[order, kind, 0, pl.ds(row, own), :] = high[:, lanes]
                    kin_s[order, kind, 1, pl.ds(row, own), :] = low[:, lanes]

    rows = count * own
    for part, target in enumerate((tr_s, ti_s)):
        one = turn_s[part * count : (part + 1) * count, :]
        target[...] = jnp.broadcast_to(one[:, None, :], (count, own, span)).reshape(rows, span)

    two = 2 * rows
    outer_high, outer_low = fwd_s.at[0:two], fwd_s.at[two : 2 * two]
    at = 2 * two
    real_high, real_low = fwd_s.at[at : at + span], fwd_s.at[at + span : at + 2 * span]
    at = at + 2 * span
    imag_high, imag_low = fwd_s.at[at : at + span], fwd_s.at[at + span : at + 2 * span]

    def by(high, low, a, full):
        total = dot(a[0], high[...])
        if len(a) > 1:
            total = total + dot(a[1], high[...])
        if full:
            total = total + dot(a[0], low[...])
        return total

    def by_real(a, full=False):
        return by(real_high, real_low, a, full)

    def by_imag(a, full=False):
        return by(imag_high, imag_low, a, full)

    def minus(a):
        return tuple(-part for part in a)

    def outer(values, full, pieces):
        g = dot(outer_high[...], values[0])
        if len(values) > 1:
            g = g + dot(outer_high[...], values[1])
        if full:
            g = g + dot(outer_low[...], values[0])
        real, imag = g[:rows], g[rows:]
        tr, ti = tr_s[...], ti_s[...]
        return pieces(real * tr - imag * ti), pieces(real * ti + imag * tr)

    for order in range(2):
        sr, si = outer((kin_s[order, 0, 0], kin_s[order, 0, 1]), True, split)
        spec_s[order, 0] = (by_real(sr, True) + by_imag(minus(si), True)) * (1.0 / length)
        dr, di = outer((kin_s[order, 1, 0], kin_s[order, 1, 1]), True, split)
        spec_s[order, 1] = (by_imag(dr, True) + by_real(di, True)) * (1.0 / length)

    def short(unit, first):
        p = recv_va[:, unit].reshape(rows, span).astype(f32)
        lane = lax.broadcasted_iota(jnp.int32, (rows, span), 1)
        none = jnp.zeros((own, span), f32)
        back = pltpu.roll(p, 1, 1)
        back = jnp.where(lane == 0, jnp.concatenate([none, back[:-own]], axis=0), back)
        ahead = pltpu.roll(p, span - 1, 1)
        ahead = jnp.where(lane == span - 1, jnp.concatenate([ahead[own:], none], axis=0), ahead)
        tap = [cols_s[:, first + i : first + i + 1] for i in range(3)]
        return (back * tap[0] + p * tap[1] + ahead * tap[2]).astype(bf16)

    def convolve(order, values, signal, pieces):
        hr, hi = outer(values, False, pieces)
        xr = by_real(hr) + by_imag(minus(hi))
        xi = by_imag(hr) + by_real(hi)
        kr, ki = spec_s[order, 0], spec_s[order, 1]
        yr = pieces(xr * kr - xi * ki)
        yi = pieces(xr * ki + xi * kr)
        ur = by_real(yr) + by_imag(yi)
        ui = by_real(yi) + by_imag(minus(yr))
        tr, ti = tr_s[...], ti_s[...]
        wr = pieces(ur * tr + ui * ti)
        wi = pieces(ui * tr - ur * ti)
        y = signal * cols_s[:, 16 + order : 17 + order]
        for part in wr:
            y = y + dot(bwd_s[0:rows, 0:rows], part)
        for part in wi:
            y = y + dot(bwd_s[0:rows, rows : 2 * rows], part)
        return y

    @pl.loop(rank + 1, count)
    def _(other):
        to = lax.rem(other + 1, count)
        pl.semaphore_wait(ready_sem.at[to], 1)
        remote_pair(to).start()

    @pl.when(has_above)
    def _():
        edge(0).start()

    @pl.when(has_below)
    def _():
        edge(1).start()

    to_all(lambda to: remote_pair(to).wait_recv())
    pieces = split if DATA_PIECES == 2 else lambda x: (x.astype(bf16),)
    value = short(0, 0)
    first_conv = convolve(0, (value,), value.astype(f32), pieces)
    gated = short(1, 8).astype(f32) * first_conv
    send_o[...] = convolve(1, pieces(gated), gated, pieces).astype(bf16)

    @pl.loop(0, count)
    def _(to):
        @pl.when(to != me)
        def _():
            remote(1, to, send_o, recv_o).start()

    mine = pl.ds(pl.multiple_of(me * own, own), own)
    recv_o[mine, :] = send_o[mine, :]

    @pl.when(has_above)
    def _():
        edge(0).wait_send()
        edge(1).wait_recv()

    @pl.when(has_below)
    def _():
        edge(1).wait_send()
        edge(0).wait_recv()

    gate = gate_s[...]
    row = lax.broadcasted_iota(jnp.int32, (span, share), 0)
    above = jnp.where(me == 0, 0.0, edge_recv[0])
    below = jnp.where(me == count - 1, 0.0, edge_recv[1])
    back = jnp.where(row == 0, above, pltpu.roll(gate, 1, 0))
    ahead = jnp.where(row == span - 1, below, pltpu.roll(gate, span - 1, 0))
    tap = taps_s[2].astype(f32)
    gate = (back * tap[0:1] + gate * tap[1:2] + ahead * tap[2:3]).astype(bf16).astype(f32)
    to_all(lambda to: remote(1, to, send_o, recv_o).wait_recv())
    out[...] = (gate * recv_o[...].astype(f32).T).astype(bf16)
    to_all(lambda to: remote_pair(to).wait_send())
    to_all(lambda to: remote(1, to, send_o, recv_o).wait_send())


def per_device(
    tokens,
    w_value,
    w_gate_a,
    w_gate_b,
    short_taps,
    pos_weight,
    pos_bias,
    sine_freq,
    hid_weight,
    hid_bias,
    filter_out,
    filter_bias,
    lag_decay,
):
    count = lax.axis_size("row")
    span, depth = tokens.shape
    share = w_value.shape[1]
    own = share // count
    rows = count * own
    hid = hid_weight.shape[0]
    feature_total = pos_weight.shape[0]
    forward, backward, turns, features = make_constants(count, own, span, feature_total)
    operands = [
        tokens,
        w_value,
        w_gate_a,
        w_gate_b,
        short_taps,
        pos_weight,
        pos_bias[None, :],
        sine_freq,
        hid_weight,
        hid_bias[None, :],
        filter_out,
        filter_bias,
        lag_decay[None, :],
        jnp.asarray(features),
        jnp.asarray(forward),
        jnp.asarray(backward),
        jnp.asarray(turns),
    ]
    cut = {4: (3, 3, share), 11: (2, share), 12: (1, share)}
    landing = [pltpu.VMEM(cut.get(i, x.shape), x.dtype) for i, x in enumerate(operands)]
    square = pltpu.VMEM((rows, span), bf16)
    scratch = [
        *landing,
        pltpu.VMEM((features.shape[0], hid), f32),
        pltpu.VMEM((24, hid), f32),
        pltpu.VMEM((32, share), f32),
        pltpu.VMEM((count, 2, own, span), bf16),
        pltpu.VMEM((count, 2, own, span), bf16),
        square,
        square,
        pltpu.VMEM((2, 1, share), f32),
        pltpu.VMEM((2, 1, share), f32),
        pltpu.VMEM((span, share), f32),
        pltpu.VMEM((rows, 32), f32),
        pltpu.VMEM((2, 2, 2, rows, span), bf16),
        pltpu.VMEM((2, 2, rows, span), f32),
        pltpu.VMEM((rows, span), f32),
        pltpu.VMEM((rows, span), f32),
        pltpu.SemaphoreType.REGULAR((count,)),
        pltpu.SemaphoreType.DMA((len(operands),)),
        pltpu.SemaphoreType.DMA((3, count)),
        pltpu.SemaphoreType.DMA((3, count)),
    ]
    return pl.pallas_call(
        functools.partial(kernel, count, own, hid, sine_coefficients()),
        out_shape=pltpu.VMEM((span, share), bf16),
        in_specs=[pl.BlockSpec(memory_space=pl.ANY)] * len(operands),
        out_specs=pl.BlockSpec(memory_space=pltpu.VMEM),
        scratch_shapes=scratch,
        compiler_params=pltpu.CompilerParams(collective_id=0, has_side_effects=True),
        name="gated_conv",
    )(*operands)


def solution(mesh):
    in_specs = (
        P(("grp", "row"), None),
        P(None, "col"),
        P(None, "col"),
        P(None, "col"),
        P(),
        P(),
        P(),
        P(),
        P(),
        P(),
        P(None, None, None, "col"),
        P(),
        P(),
    )
    out_specs = P(("grp", "row"), "col")
    return jax.shard_map(
        per_device, mesh=mesh, in_specs=in_specs, out_specs=out_specs, check_vma=False
    )
```

```python
import functools
import math

import jax
import jax.numpy as jnp
import numpy as np
from jax import lax
from jax.experimental import pallas as pl
from jax.experimental.pallas import tpu as pltpu
from jax.sharding import PartitionSpec as P

WINDOW_SHIFT = 0.05
MESH = pl.DeviceIdType.MESH
f32 = jnp.float32
bf16 = jnp.bfloat16
SIN_TERMS = 7
DATA_PIECES = 2
LATE = 6


def sine_coefficients():
    nodes = 0.5 * np.cos((np.arange(400) + 0.5) * np.pi / 800)
    basis = np.polynomial.chebyshev.Chebyshev.fit(
        nodes * nodes, np.sin(2 * np.pi * nodes) / nodes, SIN_TERMS - 1, domain=[0, 0.25]
    )
    return [float(c) for c in basis.convert(kind=np.polynomial.Polynomial).coef]


def halves(values):
    high = values.astype(jnp.bfloat16)
    low = (values - high.astype(np.float32)).astype(jnp.bfloat16)
    return high, low


def make_constants(count, own, span, feature_total):
    length = count * span
    k1 = np.arange(count)[:, None] + 0.25
    outer = np.exp(2j * np.pi * k1 * np.arange(count)[None, :] / count)
    eye = np.eye(own)
    outer_rows = np.concatenate([np.kron(outer.real, eye), np.kron(outer.imag, eye)], axis=0)
    q = np.arange(span)
    inner = np.exp(2j * np.pi * (q[:, None] * q[None, :] % span) / span)
    turn = np.exp(2j * np.pi * k1 * q[None, :] / length)
    pieces = [*halves(outer_rows.astype(np.float32))]
    for part in (inner.real, inner.imag):
        pieces += [*halves(part.astype(np.float32))]
    forward = np.concatenate(pieces, axis=0)
    backward = np.concatenate([*halves(outer_rows.T.astype(np.float32))], axis=0)
    turns = np.concatenate([turn.real, turn.imag], axis=0).astype(np.float32)
    positions = np.arange(length, dtype=np.float64)
    bands = (feature_total - 1) // 2
    frequencies = np.linspace(1e-4, bands - 1, bands)
    angles = (2.0 * math.pi / length * positions)[None, :] * frequencies[:, None]
    features = np.concatenate(
        [positions[None, :] / max(length - 1, 1), np.cos(angles), -np.sin(angles)], axis=0
    )
    padded = -(-feature_total // 16) * 16
    table = np.zeros((padded, length), np.float32)
    table[:feature_total] = features
    return forward, backward, turns, np.concatenate([*halves(table)], axis=0)


def dot(a, b):
    return jnp.dot(a, b, preferred_element_type=f32)


def dot_nt(a, b):
    return lax.dot_general(a, b, (((1,), (1,)), ((), ())), preferred_element_type=f32)


def split(values):
    high = values.astype(bf16)
    return high, (values - high.astype(f32)).astype(bf16)


def pick(selector, table):
    high = table.astype(bf16)
    rest = table - high.astype(f32)
    middle = rest.astype(bf16)
    low = (rest - middle.astype(f32)).astype(bf16)
    return dot_nt(selector, high) + dot_nt(selector, middle) + dot_nt(selector, low)


def one_hot(rows, columns, first, own):
    row = lax.broadcasted_iota(jnp.int32, (rows, columns), 0)
    column = lax.broadcasted_iota(jnp.int32, (rows, columns), 1)
    return jnp.where(column == first + row % own, 1.0, 0.0).astype(bf16)


def sine_of_turns(turns, coefficients):
    u = turns - jnp.round(turns)
    square = u * u
    total = jnp.full_like(u, coefficients[-1])
    for c in coefficients[-2::-1]:
        total = total * square + c
    return total * u


def kernel(
    count,
    own,
    hid,
    coefficients,
    tokens,
    w_value,
    w_gate_a,
    w_gate_b,
    short_taps,
    pos_weight,
    pos_bias,
    sine_freq,
    hid_weight,
    hid_bias,
    filter_out,
    filter_bias,
    lag_decay,
    features,
    forward,
    backward,
    turns,
    out,
    tok_s,
    wv_s,
    wa_s,
    wb_s,
    taps_s,
    pw_s,
    pb_s,
    sf_s,
    hw_s,
    hb_s,
    fo_s,
    fb_s,
    ld_s,
    feat_s,
    fwd_s,
    bwd_s,
    turn_s,
    pw2_s,
    np_s,
    chan_s,
    send_v,
    recv_v,
    send_a,
    recv_a,
    send_o,
    recv_o,
    edge_send,
    edge_recv,
    gate_s,
    cols_s,
    kin_s,
    spec_s,
    tr_s,
    ti_s,
    ready_sem,
    local_sem,
    send_sem,
    recv_sem,
):
    me = lax.axis_index("row")
    col = lax.axis_index("col")
    span = tok_s.shape[0]
    share = wv_s.shape[1]
    length = count * span
    barrier = pltpu.get_barrier_semaphore()

    has_below = me > 0
    has_above = me < count - 1
    turn_of_first = max(count - 5, 0)

    def rank_of(place):
        return jnp.where(place == 0, turn_of_first, place - jnp.where(place <= turn_of_first, 1, 0))

    def place_of(turn):
        return jnp.where(turn == turn_of_first, 0, turn + jnp.where(turn < turn_of_first, 1, 0))

    rank = rank_of(me)

    def signal(semaphore, to):
        pl.semaphore_signal(semaphore, inc=1, device_id={"row": to}, device_id_type=MESH)

    start = pl.multiple_of(col * share, share)
    loads = [
        (tokens, tok_s),
        (w_value, wv_s),
        (w_gate_a, wa_s),
        (w_gate_b, wb_s),
        (short_taps.at[:, :, pl.ds(start, share)], taps_s),
        (pos_weight, pw_s),
        (pos_bias, pb_s),
        (sine_freq, sf_s),
        (hid_weight, hw_s),
        (hid_bias, hb_s),
        (filter_out, fo_s),
        (filter_bias.at[:, pl.ds(start, share)], fb_s),
        (lag_decay.at[:, pl.ds(start, share)], ld_s),
        (features, feat_s),
        (forward, fwd_s),
        (backward, bwd_s),
        (turns, turn_s),
    ]
    copies = [pltpu.make_async_copy(s, t, local_sem.at[i]) for i, (s, t) in enumerate(loads)]
    for c in copies[:3]:
        c.start()

    @pl.loop(rank + 1, count)
    def _(other):
        signal(barrier, place_of(other))

    @pl.when(rank > 0)
    def _():
        pl.semaphore_wait(barrier, rank)

    @pl.loop(0, rank)
    def _(other):
        signal(ready_sem.at[me], place_of(other))

    def remote(unit, to, source, target):
        d = lax.rem(to - me + count, count)
        return pltpu.make_async_remote_copy(
            src_ref=source.at[pl.ds(pl.multiple_of(to * own, own), own)],
            dst_ref=target.at[pl.ds(pl.multiple_of(me * own, own), own)],
            send_sem=send_sem.at[unit, d],
            recv_sem=recv_sem.at[unit, d],
            device_id={"row": to},
            device_id_type=MESH,
        )

    def to_all(body):
        @pl.loop(1, count)
        def _(d):
            body(lax.rem(me + d, count))

    copies[0].wait()
    copies[1].wait()
    for c in copies[3:]:
        c.start()
    mine = pl.ds(pl.multiple_of(me * own, own), own)

    def to_lower(unit, source, target):
        @pl.loop(0, count - 1)
        def _(i):
            d = lax.div(i, 2) + 1
            to = lax.rem(me + jnp.where(lax.rem(i, 2) == 0, d, count - d), count)

            @pl.when(rank_of(to) < rank)
            def _():
                remote(unit, to, source, target).start()

        target[mine, :] = source[mine, :]

    send_v[...] = dot(tok_s[...], wv_s[...]).T.astype(bf16)
    to_lower(0, send_v, recv_v)
    copies[2].wait()
    send_a[...] = dot(tok_s[...], wa_s[...]).T.astype(bf16)
    to_lower(1, send_a, recv_a)

    def edge(side):
        return pltpu.make_async_remote_copy(
            src_ref=edge_send.at[side],
            dst_ref=edge_recv.at[side],
            send_sem=send_sem.at[3, side],
            recv_sem=recv_sem.at[3, side],
            device_id={"row": me + (1 if side == 0 else -1)},
            device_id_type=MESH,
        )

    rows = count * own
    two = 2 * rows
    outer_high, outer_low = fwd_s.at[0:two], fwd_s.at[two : 2 * two]
    at = 2 * two
    real_high, real_low = fwd_s.at[at : at + span], fwd_s.at[at + span : at + 2 * span]
    at = at + 2 * span
    imag_high, imag_low = fwd_s.at[at : at + span], fwd_s.at[at + span : at + 2 * span]

    def by(high, low, a, full):
        total = dot(a[0], high[...])
        if len(a) > 1:
            total = total + dot(a[1], high[...])
        if full:
            total = total + dot(a[0], low[...])
        return total

    def by_real(a, full=False):
        return by(real_high, real_low, a, full)

    def by_imag(a, full=False):
        return by(imag_high, imag_low, a, full)

    def minus(a):
        return tuple(-part for part in a)

    def outer(values, full, pieces):
        g = dot(outer_high[...], values[0])
        if len(values) > 1:
            g = g + dot(outer_high[...], values[1])
        if full:
            g = g + dot(outer_low[...], values[0])
        real, imag = g[:rows], g[rows:]
        tr, ti = tr_s[...], ti_s[...]
        return pieces(real * tr - imag * ti), pieces(real * ti + imag * tr)

    def prepare():
        copies[3].wait()
        gate = dot(tok_s[...], wb_s[...]).astype(bf16).astype(f32)
        gate_s[...] = gate
        edge_send[0] = gate[span - 1 : span, :]
        edge_send[1] = gate[0:1, :]

        for c in copies[4:]:
            c.wait()

        chan_s[...] = jnp.zeros_like(chan_s)
        chan_s[0:3, :] = taps_s[0].astype(f32)
        chan_s[8:11, :] = taps_s[1].astype(f32)
        chan_s[16:18, :] = fb_s[...]
        chan_s[24:25, :] = ld_s[...]
        cols_s[...] = pick(one_hot(count * own, share, me * own, own), chan_s[...])
        hid_eye = one_hot(hid, hid, 0, hid)
        feature_total = pw_s.shape[0]
        padded = feat_s.shape[0] // 2
        pw2_s[...] = jnp.zeros_like(pw2_s)
        pw2_s[0:feature_total, :] = pw_s[...]
        pw2_s[padded : padded + feature_total, :] = pw_s[...]
        np_s[...] = jnp.zeros_like(np_s)
        np_s[0:2, :] = sf_s[...]
        np_s[8:9, :] = pb_s[...]
        np_s[16:17, :] = hb_s[...]
        net = pick(hid_eye, np_s[...])
        scale_a = net[:, 0:1] * (0.5 / math.pi)
        scale_b = net[:, 1:2] * (0.5 / math.pi)
        shift_a = net[:, 8:9] * scale_a
        shift_b = net[:, 16:17] * scale_b
        first_high, first_low = split(pick(hid_eye, pw2_s[...]))
        first_low = first_low[:, :padded]

        def three(table):
            high, low = split(table)
            lane = lax.broadcasted_iota(jnp.int32, table.shape, 1)
            return jnp.where(lane < 2 * hid, high.astype(f32), low.astype(f32)).astype(bf16)

        hw = hw_s[...]
        second = three(pick(hid_eye, jnp.concatenate([hw, hw, hw], axis=0)))
        own_hot = one_hot(own, share, me * own, own)
        weights = []
        for order in range(2):
            for side in range(2):
                w = fo_s[:, order, side, :]
                weights.append(pick(own_hot, jnp.concatenate([w, w, w], axis=0)))
        third = three(jnp.concatenate(weights, axis=0))
        decay = cols_s[0:own, 24:25]

        blocks = 4
        width = length // blocks

        @pl.loop(0, blocks)
        def _(block):
            base = pl.multiple_of(block * width, width)
            feats = feat_s[:, pl.ds(base, width)]
            pre = dot(first_high, feats) + dot(first_low, feats[:padded])
            hidden = sine_of_turns(pre * scale_a + shift_a, coefficients)
            high, low = split(hidden)
            pre = dot(second, jnp.concatenate([high, low, high], axis=0))
            hidden = sine_of_turns(pre * scale_b + shift_b, coefficients)
            high, low = split(hidden)
            raw = dot(third, jnp.concatenate([high, low, high], axis=0))
            position = base + lax.broadcasted_iota(jnp.int32, (own, width), 1)
            scaled = position.astype(f32) * (1.0 / max(length - 1, 1))
            envelope = jnp.exp(-scaled * decay) + WINDOW_SHIFT
            later = jnp.where(position == 0, 0.0, envelope)
            for order in range(2):
                ahead = raw[2 * order * own : (2 * order + 1) * own] * envelope
                behind = raw[(2 * order + 1) * own : (2 * order + 2) * own] * later
                for kind, both in enumerate((ahead + behind, ahead - behind)):
                    high, low = split(both)
                    for part in range(width // span):
                        row = pl.multiple_of(block * (width // span) * own + part * own, own)
                        lanes = slice(part * span, (part + 1) * span)
                        kin_s[order, kind, 0, pl.ds(row, own), :] = high[:, lanes]
                        kin_s[order, kind, 1, pl.ds(row, own), :] = low[:, lanes]

        for part, target in enumerate((tr_s, ti_s)):
            one = turn_s[part * count : (part + 1) * count, :]
            target[...] = jnp.broadcast_to(one[:, None, :], (count, own, span)).reshape(rows, span)

        for order in range(2):
            sr, si = outer((kin_s[order, 0, 0], kin_s[order, 0, 1]), True, split)
            spec_s[order, 0] = (by_real(sr, True) + by_imag(minus(si), True)) * (1.0 / length)
            dr, di = outer((kin_s[order, 1, 0], kin_s[order, 1, 1]), True, split)
            spec_s[order, 1] = (by_imag(dr, True) + by_real(di, True)) * (1.0 / length)

    def short(ref, first):
        p = ref[...].astype(f32)
        lane = lax.broadcasted_iota(jnp.int32, (rows, span), 1)
        none = jnp.zeros((own, span), f32)
        back = pltpu.roll(p, 1, 1)
        back = jnp.where(lane == 0, jnp.concatenate([none, back[:-own]], axis=0), back)
        ahead = pltpu.roll(p, span - 1, 1)
        ahead = jnp.where(lane == span - 1, jnp.concatenate([ahead[own:], none], axis=0), ahead)
        tap = [cols_s[:, first + i : first + i + 1] for i in range(3)]
        return (back * tap[0] + p * tap[1] + ahead * tap[2]).astype(bf16)

    def convolve(order, values, signal, pieces):
        hr, hi = outer(values, False, pieces)
        xr = by_real(hr) + by_imag(minus(hi))
        xi = by_imag(hr) + by_real(hi)
        kr, ki = spec_s[order, 0], spec_s[order, 1]
        yr = pieces(xr * kr - xi * ki)
        yi = pieces(xr * ki + xi * kr)
        ur = by_real(yr) + by_imag(yi)
        ui = by_real(yi) + by_imag(minus(yr))
        tr, ti = tr_s[...], ti_s[...]
        wr = pieces(ur * tr + ui * ti)
        wi = pieces(ui * tr - ur * ti)
        y = signal * cols_s[:, 16 + order : 17 + order]
        for part in wr:
            y = y + dot(bwd_s[0:rows, 0:rows], part)
        for part in wi:
            y = y + dot(bwd_s[0:rows, rows : 2 * rows], part)
        return y

    late = (rank >= count - LATE).astype(jnp.int32)

    @pl.loop(0, 2)
    def _(step):
        pl.when(step == late)(prepare)

        @pl.when(step != late)
        def _():
            @pl.loop(rank + 1, count)
            def _(other):
                to = place_of(other)
                pl.semaphore_wait(ready_sem.at[to], 1)
                remote(0, to, send_v, recv_v).start()
                remote(1, to, send_a, recv_a).start()

    @pl.when(has_above)
    def _():
        edge(0).start()

    @pl.when(has_below)
    def _():
        edge(1).start()

    to_all(lambda to: remote(0, to, send_v, recv_v).wait_recv())
    pieces = split if DATA_PIECES == 2 else lambda x: (x.astype(bf16),)
    value = short(recv_v, 0)
    first_conv = convolve(0, (value,), value.astype(f32), pieces)
    to_all(lambda to: remote(1, to, send_a, recv_a).wait_recv())
    gated = short(recv_a, 8).astype(f32) * first_conv
    send_o[...] = convolve(1, pieces(gated), gated, pieces).astype(bf16)

    @pl.loop(0, count)
    def _(to):
        @pl.when(to != me)
        def _():
            remote(2, to, send_o, recv_o).start()

    recv_o[mine, :] = send_o[mine, :]

    @pl.when(has_above)
    def _():
        edge(0).wait_send()
        edge(1).wait_recv()

    @pl.when(has_below)
    def _():
        edge(1).wait_send()
        edge(0).wait_recv()

    gate = gate_s[...]
    row = lax.broadcasted_iota(jnp.int32, (span, share), 0)
    above = jnp.where(me == 0, 0.0, edge_recv[0])
    below = jnp.where(me == count - 1, 0.0, edge_recv[1])
    back = jnp.where(row == 0, above, pltpu.roll(gate, 1, 0))
    ahead = jnp.where(row == span - 1, below, pltpu.roll(gate, span - 1, 0))
    tap = taps_s[2].astype(f32)
    gate = (back * tap[0:1] + gate * tap[1:2] + ahead * tap[2:3]).astype(bf16).astype(f32)
    to_all(lambda to: remote(0, to, send_v, recv_v).wait_send())
    to_all(lambda to: remote(1, to, send_a, recv_a).wait_send())
    to_all(lambda to: remote(2, to, send_o, recv_o).wait_send())
    to_all(lambda to: remote(2, to, send_o, recv_o).wait_recv())
    out[...] = (gate * recv_o[...].astype(f32).T).astype(bf16)


def per_device(
    tokens,
    w_value,
    w_gate_a,
    w_gate_b,
    short_taps,
    pos_weight,
    pos_bias,
    sine_freq,
    hid_weight,
    hid_bias,
    filter_out,
    filter_bias,
    lag_decay,
):
    count = lax.axis_size("row")
    span, depth = tokens.shape
    share = w_value.shape[1]
    own = share // count
    rows = count * own
    hid = hid_weight.shape[0]
    feature_total = pos_weight.shape[0]
    forward, backward, turns, features = make_constants(count, own, span, feature_total)
    operands = [
        tokens,
        w_value,
        w_gate_a,
        w_gate_b,
        short_taps,
        pos_weight,
        pos_bias[None, :],
        sine_freq,
        hid_weight,
        hid_bias[None, :],
        filter_out,
        filter_bias,
        lag_decay[None, :],
        jnp.asarray(features),
        jnp.asarray(forward),
        jnp.asarray(backward),
        jnp.asarray(turns),
    ]
    cut = {4: (3, 3, share), 11: (2, share), 12: (1, share)}
    landing = [pltpu.VMEM(cut.get(i, x.shape), x.dtype) for i, x in enumerate(operands)]
    square = pltpu.VMEM((rows, span), bf16)
    scratch = [
        *landing,
        pltpu.VMEM((features.shape[0], hid), f32),
        pltpu.VMEM((24, hid), f32),
        pltpu.VMEM((32, share), f32),
        square,
        square,
        square,
        square,
        square,
        square,
        pltpu.VMEM((2, 1, share), f32),
        pltpu.VMEM((2, 1, share), f32),
        pltpu.VMEM((span, share), f32),
        pltpu.VMEM((rows, 32), f32),
        pltpu.VMEM((2, 2, 2, rows, span), bf16),
        pltpu.VMEM((2, 2, rows, span), f32),
        pltpu.VMEM((rows, span), f32),
        pltpu.VMEM((rows, span), f32),
        pltpu.SemaphoreType.REGULAR((count,)),
        pltpu.SemaphoreType.DMA((len(operands),)),
        pltpu.SemaphoreType.DMA((4, count)),
        pltpu.SemaphoreType.DMA((4, count)),
    ]
    return pl.pallas_call(
        functools.partial(kernel, count, own, hid, sine_coefficients()),
        out_shape=pltpu.VMEM((span, share), bf16),
        in_specs=[pl.BlockSpec(memory_space=pl.ANY)] * len(operands),
        out_specs=pl.BlockSpec(memory_space=pltpu.VMEM),
        scratch_shapes=scratch,
        compiler_params=pltpu.CompilerParams(collective_id=0, has_side_effects=True),
        name="gated_conv",
    )(*operands)


def solution(mesh):
    in_specs = (
        P(("grp", "row"), None),
        P(None, "col"),
        P(None, "col"),
        P(None, "col"),
        P(),
        P(),
        P(),
        P(),
        P(),
        P(),
        P(None, None, None, "col"),
        P(),
        P(),
    )
    out_specs = P(("grp", "row"), "col")
    return jax.shard_map(
        per_device, mesh=mesh, in_specs=in_specs, out_specs=out_specs, check_vma=False
    )
```

```python
import functools
import math

import jax
import jax.numpy as jnp
import numpy as np
from jax import lax
from jax.experimental import pallas as pl
from jax.experimental.pallas import tpu as pltpu
from jax.sharding import PartitionSpec as P

WINDOW_SHIFT = 0.05
MESH = pl.DeviceIdType.MESH
f32 = jnp.float32
bf16 = jnp.bfloat16
SIN_TERMS = 7
DATA_PIECES = 2


def sine_coefficients():
    nodes = 0.5 * np.cos((np.arange(400) + 0.5) * np.pi / 800)
    basis = np.polynomial.chebyshev.Chebyshev.fit(
        nodes * nodes, np.sin(2 * np.pi * nodes) / nodes, SIN_TERMS - 1, domain=[0, 0.25]
    )
    return [float(c) for c in basis.convert(kind=np.polynomial.Polynomial).coef]


def halves(values):
    high = values.astype(jnp.bfloat16)
    low = (values - high.astype(np.float32)).astype(jnp.bfloat16)
    return high, low


def make_constants(count, own, span, feature_total):
    length = count * span
    k1 = np.arange(count)[:, None] + 0.25
    outer = np.exp(2j * np.pi * k1 * np.arange(count)[None, :] / count)
    eye = np.eye(own)
    outer_rows = np.concatenate([np.kron(outer.real, eye), np.kron(outer.imag, eye)], axis=0)
    q = np.arange(span)
    inner = np.exp(2j * np.pi * (q[:, None] * q[None, :] % span) / span)
    turn = np.exp(2j * np.pi * k1 * q[None, :] / length)
    pieces = [*halves(outer_rows.astype(np.float32))]
    for part in (inner.real, inner.imag):
        pieces += [*halves(part.astype(np.float32))]
    forward = np.concatenate(pieces, axis=0)
    backward = np.concatenate([*halves(outer_rows.T.astype(np.float32))], axis=0)
    turns = np.concatenate([turn.real, turn.imag], axis=0).astype(np.float32)
    positions = np.arange(length, dtype=np.float64)
    bands = (feature_total - 1) // 2
    frequencies = np.linspace(1e-4, bands - 1, bands)
    angles = (2.0 * math.pi / length * positions)[None, :] * frequencies[:, None]
    features = np.concatenate(
        [positions[None, :] / max(length - 1, 1), np.cos(angles), -np.sin(angles)], axis=0
    )
    padded = -(-feature_total // 16) * 16
    table = np.zeros((padded, length), np.float32)
    table[:feature_total] = features
    return forward, backward, turns, np.concatenate([*halves(table)], axis=0)


def dot(a, b):
    return jnp.dot(a, b, preferred_element_type=f32)


def dot_nt(a, b):
    return lax.dot_general(a, b, (((1,), (1,)), ((), ())), preferred_element_type=f32)


def split(values):
    high = values.astype(bf16)
    return high, (values - high.astype(f32)).astype(bf16)


def pick(selector, table):
    high = table.astype(bf16)
    rest = table - high.astype(f32)
    middle = rest.astype(bf16)
    low = (rest - middle.astype(f32)).astype(bf16)
    return dot_nt(selector, high) + dot_nt(selector, middle) + dot_nt(selector, low)


def one_hot(rows, columns, first, own):
    row = lax.broadcasted_iota(jnp.int32, (rows, columns), 0)
    column = lax.broadcasted_iota(jnp.int32, (rows, columns), 1)
    return jnp.where(column == first + row % own, 1.0, 0.0).astype(bf16)


def sine_of_turns(turns, coefficients):
    u = turns - jnp.round(turns)
    square = u * u
    total = jnp.full_like(u, coefficients[-1])
    for c in coefficients[-2::-1]:
        total = total * square + c
    return total * u


def kernel(
    count,
    own,
    hid,
    coefficients,
    tokens,
    w_value,
    w_gate_a,
    w_gate_b,
    short_taps,
    pos_weight,
    pos_bias,
    sine_freq,
    hid_weight,
    hid_bias,
    filter_out,
    filter_bias,
    lag_decay,
    features,
    forward,
    backward,
    turns,
    out,
    tok_s,
    wv_s,
    wa_s,
    wb_s,
    taps_s,
    pw_s,
    pb_s,
    sf_s,
    hw_s,
    hb_s,
    fo_s,
    fb_s,
    ld_s,
    feat_s,
    fwd_s,
    bwd_s,
    turn_s,
    pw2_s,
    np_s,
    chan_s,
    send_v,
    recv_v,
    send_a,
    recv_a,
    send_o,
    recv_o,
    edge_send,
    edge_recv,
    gate_s,
    cols_s,
    kin_s,
    spec_s,
    tr_s,
    ti_s,
    ready_sem,
    local_sem,
    send_sem,
    recv_sem,
):
    me = lax.axis_index("row")
    col = lax.axis_index("col")
    span = tok_s.shape[0]
    share = wv_s.shape[1]
    length = count * span
    barrier = pltpu.get_barrier_semaphore()

    has_below = me > 0
    has_above = me < count - 1
    turn_of_first = max(count - 5, 0)

    def rank_of(place):
        return jnp.where(place == 0, turn_of_first, place - jnp.where(place <= turn_of_first, 1, 0))

    def place_of(turn):
        return jnp.where(turn == turn_of_first, 0, turn + jnp.where(turn < turn_of_first, 1, 0))

    rank = rank_of(me)

    def signal(semaphore, to):
        pl.semaphore_signal(semaphore, inc=1, device_id={"row": to}, device_id_type=MESH)

    start = pl.multiple_of(col * share, share)
    loads = [
        (tokens, tok_s),
        (w_value, wv_s),
        (w_gate_a, wa_s),
        (w_gate_b, wb_s),
        (short_taps.at[:, :, pl.ds(start, share)], taps_s),
        (pos_weight, pw_s),
        (pos_bias, pb_s),
        (sine_freq, sf_s),
        (hid_weight, hw_s),
        (hid_bias, hb_s),
        (filter_out, fo_s),
        (filter_bias.at[:, pl.ds(start, share)], fb_s),
        (lag_decay.at[:, pl.ds(start, share)], ld_s),
        (features, feat_s),
        (forward, fwd_s),
        (backward, bwd_s),
        (turns, turn_s),
    ]
    copies = [pltpu.make_async_copy(s, t, local_sem.at[i]) for i, (s, t) in enumerate(loads)]
    for c in copies[:3]:
        c.start()

    @pl.loop(rank + 1, count)
    def _(other):
        signal(barrier, place_of(other))

    @pl.when(rank > 0)
    def _():
        pl.semaphore_wait(barrier, rank)

    @pl.loop(0, rank)
    def _(other):
        signal(ready_sem.at[me], place_of(other))

    def remote(unit, to, source, target):
        d = lax.rem(to - me + count, count)
        return pltpu.make_async_remote_copy(
            src_ref=source.at[pl.ds(pl.multiple_of(to * own, own), own)],
            dst_ref=target.at[pl.ds(pl.multiple_of(me * own, own), own)],
            send_sem=send_sem.at[unit, d],
            recv_sem=recv_sem.at[unit, d],
            device_id={"row": to},
            device_id_type=MESH,
        )

    def to_all(body):
        @pl.loop(1, count)
        def _(d):
            body(lax.rem(me + d, count))

    copies[0].wait()
    copies[1].wait()
    for c in copies[3:]:
        c.start()
    mine = pl.ds(pl.multiple_of(me * own, own), own)

    def to_lower(unit, source, target):
        @pl.loop(0, count - 1)
        def _(i):
            d = lax.div(i, 2) + 1
            to = lax.rem(me + jnp.where(lax.rem(i, 2) == 0, d, count - d), count)

            @pl.when(rank_of(to) < rank)
            def _():
                remote(unit, to, source, target).start()

        target[mine, :] = source[mine, :]

    send_v[...] = dot(tok_s[...], wv_s[...]).T.astype(bf16)
    to_lower(0, send_v, recv_v)
    copies[2].wait()
    send_a[...] = dot(tok_s[...], wa_s[...]).T.astype(bf16)
    to_lower(1, send_a, recv_a)

    def edge(side):
        return pltpu.make_async_remote_copy(
            src_ref=edge_send.at[side],
            dst_ref=edge_recv.at[side],
            send_sem=send_sem.at[3, side],
            recv_sem=recv_sem.at[3, side],
            device_id={"row": me + (1 if side == 0 else -1)},
            device_id_type=MESH,
        )

    rows = count * own
    two = 2 * rows
    outer_high, outer_low = fwd_s.at[0:two], fwd_s.at[two : 2 * two]
    at = 2 * two
    real_high, real_low = fwd_s.at[at : at + span], fwd_s.at[at + span : at + 2 * span]
    at = at + 2 * span
    imag_high, imag_low = fwd_s.at[at : at + span], fwd_s.at[at + span : at + 2 * span]

    def by(high, low, a, full):
        total = dot(a[0], high[...])
        if len(a) > 1:
            total = total + dot(a[1], high[...])
        if full:
            total = total + dot(a[0], low[...])
        return total

    def by_real(a, full=False):
        return by(real_high, real_low, a, full)

    def by_imag(a, full=False):
        return by(imag_high, imag_low, a, full)

    def minus(a):
        return tuple(-part for part in a)

    def outer(values, full, pieces):
        g = dot(outer_high[...], values[0])
        if len(values) > 1:
            g = g + dot(outer_high[...], values[1])
        if full:
            g = g + dot(outer_low[...], values[0])
        real, imag = g[:rows], g[rows:]
        tr, ti = tr_s[...], ti_s[...]
        return pieces(real * tr - imag * ti), pieces(real * ti + imag * tr)

    def serve(turn):
        to = place_of(turn)
        pl.semaphore_wait(ready_sem.at[to], 1)
        remote(0, to, send_v, recv_v).start()
        remote(1, to, send_a, recv_a).start()

    def serve_next(steps):
        pl.when(rank + steps < count)(lambda: serve(rank + steps))

    def prepare():
        serve_next(1)
        serve_next(2)
        copies[3].wait()
        gate = dot(tok_s[...], wb_s[...]).astype(bf16).astype(f32)
        gate_s[...] = gate
        edge_send[0] = gate[span - 1 : span, :]
        edge_send[1] = gate[0:1, :]

        for c in copies[4:]:
            c.wait()

        chan_s[...] = jnp.zeros_like(chan_s)
        chan_s[0:3, :] = taps_s[0].astype(f32)
        chan_s[8:11, :] = taps_s[1].astype(f32)
        chan_s[16:18, :] = fb_s[...]
        chan_s[24:25, :] = ld_s[...]
        cols_s[...] = pick(one_hot(count * own, share, me * own, own), chan_s[...])
        hid_eye = one_hot(hid, hid, 0, hid)
        feature_total = pw_s.shape[0]
        padded = feat_s.shape[0] // 2
        pw2_s[...] = jnp.zeros_like(pw2_s)
        pw2_s[0:feature_total, :] = pw_s[...]
        pw2_s[padded : padded + feature_total, :] = pw_s[...]
        np_s[...] = jnp.zeros_like(np_s)
        np_s[0:2, :] = sf_s[...]
        np_s[8:9, :] = pb_s[...]
        np_s[16:17, :] = hb_s[...]
        net = pick(hid_eye, np_s[...])
        scale_a = net[:, 0:1] * (0.5 / math.pi)
        scale_b = net[:, 1:2] * (0.5 / math.pi)
        shift_a = net[:, 8:9] * scale_a
        shift_b = net[:, 16:17] * scale_b
        first_high, first_low = split(pick(hid_eye, pw2_s[...]))
        first_low = first_low[:, :padded]

        def three(table):
            high, low = split(table)
            lane = lax.broadcasted_iota(jnp.int32, table.shape, 1)
            return jnp.where(lane < 2 * hid, high.astype(f32), low.astype(f32)).astype(bf16)

        hw = hw_s[...]
        second = three(pick(hid_eye, jnp.concatenate([hw, hw, hw], axis=0)))
        own_hot = one_hot(own, share, me * own, own)
        weights = []
        for order in range(2):
            for side in range(2):
                w = fo_s[:, order, side, :]
                weights.append(pick(own_hot, jnp.concatenate([w, w, w], axis=0)))
        third = three(jnp.concatenate(weights, axis=0))
        decay = cols_s[0:own, 24:25]

        serve_next(3)

        blocks = 4
        width = length // blocks

        @pl.loop(0, blocks)
        def _(block):
            base = pl.multiple_of(block * width, width)
            feats = feat_s[:, pl.ds(base, width)]
            pre = dot(first_high, feats) + dot(first_low, feats[:padded])
            hidden = sine_of_turns(pre * scale_a + shift_a, coefficients)
            high, low = split(hidden)
            pre = dot(second, jnp.concatenate([high, low, high], axis=0))
            hidden = sine_of_turns(pre * scale_b + shift_b, coefficients)
            high, low = split(hidden)
            raw = dot(third, jnp.concatenate([high, low, high], axis=0))
            position = base + lax.broadcasted_iota(jnp.int32, (own, width), 1)
            scaled = position.astype(f32) * (1.0 / max(length - 1, 1))
            envelope = jnp.exp(-scaled * decay) + WINDOW_SHIFT
            later = jnp.where(position == 0, 0.0, envelope)
            for order in range(2):
                ahead = raw[2 * order * own : (2 * order + 1) * own] * envelope
                behind = raw[(2 * order + 1) * own : (2 * order + 2) * own] * later
                for kind, both in enumerate((ahead + behind, ahead - behind)):
                    high, low = split(both)
                    for part in range(width // span):
                        row = pl.multiple_of(block * (width // span) * own + part * own, own)
                        lanes = slice(part * span, (part + 1) * span)
                        kin_s[order, kind, 0, pl.ds(row, own), :] = high[:, lanes]
                        kin_s[order, kind, 1, pl.ds(row, own), :] = low[:, lanes]

            @pl.when(lax.rem(block, 2) == 1)
            def _():
                serve_next(4 + lax.div(block, 2))

        for part, target in enumerate((tr_s, ti_s)):
            one = turn_s[part * count : (part + 1) * count, :]
            target[...] = jnp.broadcast_to(one[:, None, :], (count, own, span)).reshape(rows, span)

        for order in range(2):
            sr, si = outer((kin_s[order, 0, 0], kin_s[order, 0, 1]), True, split)
            spec_s[order, 0] = (by_real(sr, True) + by_imag(minus(si), True)) * (1.0 / length)
            dr, di = outer((kin_s[order, 1, 0], kin_s[order, 1, 1]), True, split)
            spec_s[order, 1] = (by_imag(dr, True) + by_real(di, True)) * (1.0 / length)
            if order == 0:
                serve_next(6)

    def short(ref, first):
        p = ref[...].astype(f32)
        lane = lax.broadcasted_iota(jnp.int32, (rows, span), 1)
        none = jnp.zeros((own, span), f32)
        back = pltpu.roll(p, 1, 1)
        back = jnp.where(lane == 0, jnp.concatenate([none, back[:-own]], axis=0), back)
        ahead = pltpu.roll(p, span - 1, 1)
        ahead = jnp.where(lane == span - 1, jnp.concatenate([ahead[own:], none], axis=0), ahead)
        tap = [cols_s[:, first + i : first + i + 1] for i in range(3)]
        return (back * tap[0] + p * tap[1] + ahead * tap[2]).astype(bf16)

    def convolve(order, values, signal, pieces):
        hr, hi = outer(values, False, pieces)
        xr = by_real(hr) + by_imag(minus(hi))
        xi = by_imag(hr) + by_real(hi)
        kr, ki = spec_s[order, 0], spec_s[order, 1]
        yr = pieces(xr * kr - xi * ki)
        yi = pieces(xr * ki + xi * kr)
        ur = by_real(yr) + by_imag(yi)
        ui = by_real(yi) + by_imag(minus(yr))
        tr, ti = tr_s[...], ti_s[...]
        wr = pieces(ur * tr + ui * ti)
        wi = pieces(ui * tr - ur * ti)
        y = signal * cols_s[:, 16 + order : 17 + order]
        for part in wr:
            y = y + dot(bwd_s[0:rows, 0:rows], part)
        for part in wi:
            y = y + dot(bwd_s[0:rows, rows : 2 * rows], part)
        return y

    prepare()

    @pl.loop(rank + 7, count)
    def _(turn):
        serve(turn)

    @pl.when(has_above)
    def _():
        edge(0).start()

    @pl.when(has_below)
    def _():
        edge(1).start()

    to_all(lambda to: remote(0, to, send_v, recv_v).wait_recv())
    pieces = split if DATA_PIECES == 2 else lambda x: (x.astype(bf16),)
    value = short(recv_v, 0)
    first_conv = convolve(0, (value,), value.astype(f32), pieces)
    to_all(lambda to: remote(1, to, send_a, recv_a).wait_recv())
    gated = short(recv_a, 8).astype(f32) * first_conv
    send_o[...] = convolve(1, pieces(gated), gated, pieces).astype(bf16)

    @pl.loop(0, count)
    def _(to):
        @pl.when(to != me)
        def _():
            remote(2, to, send_o, recv_o).start()

    recv_o[mine, :] = send_o[mine, :]

    @pl.when(has_above)
    def _():
        edge(0).wait_send()
        edge(1).wait_recv()

    @pl.when(has_below)
    def _():
        edge(1).wait_send()
        edge(0).wait_recv()

    gate = gate_s[...]
    row = lax.broadcasted_iota(jnp.int32, (span, share), 0)
    above = jnp.where(me == 0, 0.0, edge_recv[0])
    below = jnp.where(me == count - 1, 0.0, edge_recv[1])
    back = jnp.where(row == 0, above, pltpu.roll(gate, 1, 0))
    ahead = jnp.where(row == span - 1, below, pltpu.roll(gate, span - 1, 0))
    tap = taps_s[2].astype(f32)
    gate = (back * tap[0:1] + gate * tap[1:2] + ahead * tap[2:3]).astype(bf16).astype(f32)
    to_all(lambda to: remote(0, to, send_v, recv_v).wait_send())
    to_all(lambda to: remote(1, to, send_a, recv_a).wait_send())
    to_all(lambda to: remote(2, to, send_o, recv_o).wait_send())
    to_all(lambda to: remote(2, to, send_o, recv_o).wait_recv())
    out[...] = (gate * recv_o[...].astype(f32).T).astype(bf16)


def per_device(
    tokens,
    w_value,
    w_gate_a,
    w_gate_b,
    short_taps,
    pos_weight,
    pos_bias,
    sine_freq,
    hid_weight,
    hid_bias,
    filter_out,
    filter_bias,
    lag_decay,
):
    count = lax.axis_size("row")
    span, depth = tokens.shape
    share = w_value.shape[1]
    own = share // count
    rows = count * own
    hid = hid_weight.shape[0]
    feature_total = pos_weight.shape[0]
    forward, backward, turns, features = make_constants(count, own, span, feature_total)
    operands = [
        tokens,
        w_value,
        w_gate_a,
        w_gate_b,
        short_taps,
        pos_weight,
        pos_bias[None, :],
        sine_freq,
        hid_weight,
        hid_bias[None, :],
        filter_out,
        filter_bias,
        lag_decay[None, :],
        jnp.asarray(features),
        jnp.asarray(forward),
        jnp.asarray(backward),
        jnp.asarray(turns),
    ]
    cut = {4: (3, 3, share), 11: (2, share), 12: (1, share)}
    landing = [pltpu.VMEM(cut.get(i, x.shape), x.dtype) for i, x in enumerate(operands)]
    square = pltpu.VMEM((rows, span), bf16)
    scratch = [
        *landing,
        pltpu.VMEM((features.shape[0], hid), f32),
        pltpu.VMEM((24, hid), f32),
        pltpu.VMEM((32, share), f32),
        square,
        square,
        square,
        square,
        square,
        square,
        pltpu.VMEM((2, 1, share), f32),
        pltpu.VMEM((2, 1, share), f32),
        pltpu.VMEM((span, share), f32),
        pltpu.VMEM((rows, 32), f32),
        pltpu.VMEM((2, 2, 2, rows, span), bf16),
        pltpu.VMEM((2, 2, rows, span), f32),
        pltpu.VMEM((rows, span), f32),
        pltpu.VMEM((rows, span), f32),
        pltpu.SemaphoreType.REGULAR((count,)),
        pltpu.SemaphoreType.DMA((len(operands),)),
        pltpu.SemaphoreType.DMA((4, count)),
        pltpu.SemaphoreType.DMA((4, count)),
    ]
    return pl.pallas_call(
        functools.partial(kernel, count, own, hid, sine_coefficients()),
        out_shape=pltpu.VMEM((span, share), bf16),
        in_specs=[pl.BlockSpec(memory_space=pl.ANY)] * len(operands),
        out_specs=pl.BlockSpec(memory_space=pltpu.VMEM),
        scratch_shapes=scratch,
        compiler_params=pltpu.CompilerParams(collective_id=0, has_side_effects=True),
        name="gated_conv",
    )(*operands)


def solution(mesh):
    in_specs = (
        P(("grp", "row"), None),
        P(None, "col"),
        P(None, "col"),
        P(None, "col"),
        P(),
        P(),
        P(),
        P(),
        P(),
        P(),
        P(None, None, None, "col"),
        P(),
        P(),
    )
    out_specs = P(("grp", "row"), "col")
    return jax.shard_map(
        per_device, mesh=mesh, in_specs=in_specs, out_specs=out_specs, check_vma=False
    )
```

```python
import functools
import math

import jax
import jax.numpy as jnp
import numpy as np
from jax import lax
from jax.experimental import pallas as pl
from jax.experimental.pallas import tpu as pltpu
from jax.sharding import PartitionSpec as P

WINDOW_SHIFT = 0.05
MESH = pl.DeviceIdType.MESH
f32 = jnp.float32
bf16 = jnp.bfloat16
SIN_TERMS = 7
DATA_PIECES = 2


def sine_coefficients():
    nodes = 0.5 * np.cos((np.arange(400) + 0.5) * np.pi / 800)
    basis = np.polynomial.chebyshev.Chebyshev.fit(
        nodes * nodes, np.sin(2 * np.pi * nodes) / nodes, SIN_TERMS - 1, domain=[0, 0.25]
    )
    return [float(c) for c in basis.convert(kind=np.polynomial.Polynomial).coef]


def halves(values):
    high = values.astype(jnp.bfloat16)
    low = (values - high.astype(np.float32)).astype(jnp.bfloat16)
    return high, low


def make_constants(count, own, span, feature_total):
    length = count * span
    k1 = np.arange(count)[:, None] + 0.25
    outer = np.exp(2j * np.pi * k1 * np.arange(count)[None, :] / count)
    eye = np.eye(own)
    outer_rows = np.concatenate([np.kron(outer.real, eye), np.kron(outer.imag, eye)], axis=0)
    q = np.arange(span)
    inner = np.exp(2j * np.pi * (q[:, None] * q[None, :] % span) / span)
    turn = np.exp(2j * np.pi * k1 * q[None, :] / length)
    pieces = [*halves(outer_rows.astype(np.float32))]
    for part in (inner.real, inner.imag):
        pieces += [*halves(part.astype(np.float32))]
    forward = np.concatenate(pieces, axis=0)
    backward = np.concatenate([*halves(outer_rows.T.astype(np.float32))], axis=0)
    turns = np.concatenate([turn.real, turn.imag], axis=0).astype(np.float32)
    positions = np.arange(length, dtype=np.float64)
    bands = (feature_total - 1) // 2
    frequencies = np.linspace(1e-4, bands - 1, bands)
    angles = (2.0 * math.pi / length * positions)[None, :] * frequencies[:, None]
    features = np.concatenate(
        [positions[None, :] / max(length - 1, 1), np.cos(angles), -np.sin(angles)], axis=0
    )
    padded = -(-feature_total // 16) * 16
    table = np.zeros((padded, length), np.float32)
    table[:feature_total] = features
    return forward, backward, turns, np.concatenate([*halves(table)], axis=0)


def dot(a, b):
    return jnp.dot(a, b, preferred_element_type=f32)


def dot_nt(a, b):
    return lax.dot_general(a, b, (((1,), (1,)), ((), ())), preferred_element_type=f32)


def split(values):
    high = values.astype(bf16)
    return high, (values - high.astype(f32)).astype(bf16)


def pick(selector, table):
    high = table.astype(bf16)
    rest = table - high.astype(f32)
    middle = rest.astype(bf16)
    low = (rest - middle.astype(f32)).astype(bf16)
    return dot_nt(selector, high) + dot_nt(selector, middle) + dot_nt(selector, low)


def one_hot(rows, columns, first, own):
    row = lax.broadcasted_iota(jnp.int32, (rows, columns), 0)
    column = lax.broadcasted_iota(jnp.int32, (rows, columns), 1)
    return jnp.where(column == first + row % own, 1.0, 0.0).astype(bf16)


def sine_of_turns(turns, coefficients):
    u = turns - jnp.round(turns)
    square = u * u
    total = jnp.full_like(u, coefficients[-1])
    for c in coefficients[-2::-1]:
        total = total * square + c
    return total * u


def kernel(
    count,
    own,
    hid,
    coefficients,
    tokens,
    w_value,
    w_gate_a,
    w_gate_b,
    short_taps,
    pos_weight,
    pos_bias,
    sine_freq,
    hid_weight,
    hid_bias,
    filter_out,
    filter_bias,
    lag_decay,
    features,
    forward,
    backward,
    turns,
    out,
    tok_s,
    wv_s,
    wa_s,
    wb_s,
    taps_s,
    pw_s,
    pb_s,
    sf_s,
    hw_s,
    hb_s,
    fo_s,
    fb_s,
    ld_s,
    feat_s,
    fwd_s,
    bwd_s,
    turn_s,
    pw2_s,
    np_s,
    chan_s,
    send_v,
    recv_v,
    send_a,
    recv_a,
    send_o,
    recv_o,
    edge_send,
    edge_recv,
    gate_s,
    cols_s,
    kin_s,
    spec_s,
    tr_s,
    ti_s,
    ready_sem,
    local_sem,
    send_sem,
    recv_sem,
):
    me = lax.axis_index("row")
    col = lax.axis_index("col")
    span = tok_s.shape[0]
    share = wv_s.shape[1]
    length = count * span
    barrier = pltpu.get_barrier_semaphore()

    has_below = me > 0
    has_above = me < count - 1
    turn_of_first = max(count - 5, 0)

    def rank_of(place):
        return jnp.where(place == 0, turn_of_first, place - jnp.where(place <= turn_of_first, 1, 0))

    def place_of(turn):
        return jnp.where(turn == turn_of_first, 0, turn + jnp.where(turn < turn_of_first, 1, 0))

    rank = rank_of(me)

    def signal(semaphore, to):
        pl.semaphore_signal(semaphore, inc=1, device_id={"row": to}, device_id_type=MESH)

    start = pl.multiple_of(col * share, share)
    loads = [
        (tokens, tok_s),
        (w_value, wv_s),
        (w_gate_a, wa_s),
        (w_gate_b, wb_s),
        (short_taps.at[:, :, pl.ds(start, share)], taps_s),
        (pos_weight, pw_s),
        (pos_bias, pb_s),
        (sine_freq, sf_s),
        (hid_weight, hw_s),
        (hid_bias, hb_s),
        (filter_out, fo_s),
        (filter_bias.at[:, pl.ds(start, share)], fb_s),
        (lag_decay.at[:, pl.ds(start, share)], ld_s),
        (features, feat_s),
        (forward, fwd_s),
        (backward, bwd_s),
        (turns, turn_s),
    ]
    copies = [pltpu.make_async_copy(s, t, local_sem.at[i]) for i, (s, t) in enumerate(loads)]
    for c in copies[:3]:
        c.start()

    @pl.loop(rank + 1, count)
    def _(other):
        signal(barrier, place_of(other))

    @pl.when(rank > 0)
    def _():
        pl.semaphore_wait(barrier, rank)

    @pl.loop(0, rank)
    def _(other):
        signal(ready_sem.at[me], place_of(other))

    def remote(unit, to, source, target):
        d = lax.rem(to - me + count, count)
        return pltpu.make_async_remote_copy(
            src_ref=source.at[pl.ds(pl.multiple_of(to * own, own), own)],
            dst_ref=target.at[pl.ds(pl.multiple_of(me * own, own), own)],
            send_sem=send_sem.at[unit, d],
            recv_sem=recv_sem.at[unit, d],
            device_id={"row": to},
            device_id_type=MESH,
        )

    def to_all(body):
        @pl.loop(1, count)
        def _(d):
            body(lax.rem(me + d, count))

    copies[0].wait()
    copies[1].wait()
    for c in copies[3:]:
        c.start()
    mine = pl.ds(pl.multiple_of(me * own, own), own)

    def to_lower(unit, source, target):
        @pl.loop(0, count - 1)
        def _(i):
            step = lax.div(i + 1, 2)
            d = count // 2 + jnp.where(lax.rem(i, 2) == 1, step, -step)
            to = lax.rem(me + d, count)

            @pl.when(rank_of(to) < rank)
            def _():
                remote(unit, to, source, target).start()

        target[mine, :] = source[mine, :]

    send_v[...] = dot(tok_s[...], wv_s[...]).T.astype(bf16)
    to_lower(0, send_v, recv_v)
    copies[2].wait()
    send_a[...] = dot(tok_s[...], wa_s[...]).T.astype(bf16)
    to_lower(1, send_a, recv_a)

    def edge(side):
        return pltpu.make_async_remote_copy(
            src_ref=edge_send.at[side],
            dst_ref=edge_recv.at[side],
            send_sem=send_sem.at[3, side],
            recv_sem=recv_sem.at[3, side],
            device_id={"row": me + (1 if side == 0 else -1)},
            device_id_type=MESH,
        )

    rows = count * own
    two = 2 * rows
    outer_high, outer_low = fwd_s.at[0:two], fwd_s.at[two : 2 * two]
    at = 2 * two
    real_high, real_low = fwd_s.at[at : at + span], fwd_s.at[at + span : at + 2 * span]
    at = at + 2 * span
    imag_high, imag_low = fwd_s.at[at : at + span], fwd_s.at[at + span : at + 2 * span]

    def by(high, low, a, full):
        total = dot(a[0], high[...])
        if len(a) > 1:
            total = total + dot(a[1], high[...])
        if full:
            total = total + dot(a[0], low[...])
        return total

    def by_real(a, full=False):
        return by(real_high, real_low, a, full)

    def by_imag(a, full=False):
        return by(imag_high, imag_low, a, full)

    def minus(a):
        return tuple(-part for part in a)

    def outer(values, full, pieces):
        g = dot(outer_high[...], values[0])
        if len(values) > 1:
            g = g + dot(outer_high[...], values[1])
        if full:
            g = g + dot(outer_low[...], values[0])
        real, imag = g[:rows], g[rows:]
        tr, ti = tr_s[...], ti_s[...]
        return pieces(real * tr - imag * ti), pieces(real * ti + imag * tr)

    def serve(to):
        pl.semaphore_wait(ready_sem.at[to], 1)
        remote(0, to, send_v, recv_v).start()
        remote(1, to, send_a, recv_a).start()

    serve_base = jnp.where(me == 0, turn_of_first, me)

    def serve_next(steps):
        pl.when(serve_base + steps < count)(lambda: serve(serve_base + steps))

    def prepare():
        serve_next(1)
        serve_next(2)
        copies[3].wait()
        gate = dot(tok_s[...], wb_s[...]).astype(bf16).astype(f32)
        gate_s[...] = gate
        edge_send[0] = gate[span - 1 : span, :]
        edge_send[1] = gate[0:1, :]

        for c in copies[4:]:
            c.wait()

        chan_s[...] = jnp.zeros_like(chan_s)
        chan_s[0:3, :] = taps_s[0].astype(f32)
        chan_s[8:11, :] = taps_s[1].astype(f32)
        chan_s[16:18, :] = fb_s[...]
        chan_s[24:25, :] = ld_s[...]
        cols_s[...] = pick(one_hot(count * own, share, me * own, own), chan_s[...])
        hid_eye = one_hot(hid, hid, 0, hid)
        feature_total = pw_s.shape[0]
        padded = feat_s.shape[0] // 2
        pw2_s[...] = jnp.zeros_like(pw2_s)
        pw2_s[0:feature_total, :] = pw_s[...]
        pw2_s[padded : padded + feature_total, :] = pw_s[...]
        np_s[...] = jnp.zeros_like(np_s)
        np_s[0:2, :] = sf_s[...]
        np_s[8:9, :] = pb_s[...]
        np_s[16:17, :] = hb_s[...]
        net = pick(hid_eye, np_s[...])
        scale_a = net[:, 0:1] * (0.5 / math.pi)
        scale_b = net[:, 1:2] * (0.5 / math.pi)
        shift_a = net[:, 8:9] * scale_a
        shift_b = net[:, 16:17] * scale_b
        first_high, first_low = split(pick(hid_eye, pw2_s[...]))
        first_low = first_low[:, :padded]

        def three(table):
            high, low = split(table)
            lane = lax.broadcasted_iota(jnp.int32, table.shape, 1)
            return jnp.where(lane < 2 * hid, high.astype(f32), low.astype(f32)).astype(bf16)

        hw = hw_s[...]
        second = three(pick(hid_eye, jnp.concatenate([hw, hw, hw], axis=0)))
        own_hot = one_hot(own, share, me * own, own)
        weights = []
        for order in range(2):
            for side in range(2):
                w = fo_s[:, order, side, :]
                weights.append(pick(own_hot, jnp.concatenate([w, w, w], axis=0)))
        third = three(jnp.concatenate(weights, axis=0))
        decay = cols_s[0:own, 24:25]

        serve_next(3)

        blocks = 4
        width = length // blocks

        @pl.loop(0, blocks)
        def _(block):
            base = pl.multiple_of(block * width, width)
            feats = feat_s[:, pl.ds(base, width)]
            pre = dot(first_high, feats) + dot(first_low, feats[:padded])
            hidden = sine_of_turns(pre * scale_a + shift_a, coefficients)
            high, low = split(hidden)
            pre = dot(second, jnp.concatenate([high, low, high], axis=0))
            hidden = sine_of_turns(pre * scale_b + shift_b, coefficients)
            high, low = split(hidden)
            raw = dot(third, jnp.concatenate([high, low, high], axis=0))
            position = base + lax.broadcasted_iota(jnp.int32, (own, width), 1)
            scaled = position.astype(f32) * (1.0 / max(length - 1, 1))
            envelope = jnp.exp(-scaled * decay) + WINDOW_SHIFT
            later = jnp.where(position == 0, 0.0, envelope)
            for order in range(2):
                ahead = raw[2 * order * own : (2 * order + 1) * own] * envelope
                behind = raw[(2 * order + 1) * own : (2 * order + 2) * own] * later
                for kind, both in enumerate((ahead + behind, ahead - behind)):
                    high, low = split(both)
                    for part in range(width // span):
                        row = pl.multiple_of(block * (width // span) * own + part * own, own)
                        lanes = slice(part * span, (part + 1) * span)
                        kin_s[order, kind, 0, pl.ds(row, own), :] = high[:, lanes]
                        kin_s[order, kind, 1, pl.ds(row, own), :] = low[:, lanes]

            @pl.when(lax.rem(block, 2) == 1)
            def _():
                serve_next(4 + lax.div(block, 2))

        for part, target in enumerate((tr_s, ti_s)):
            one = turn_s[part * count : (part + 1) * count, :]
            target[...] = jnp.broadcast_to(one[:, None, :], (count, own, span)).reshape(rows, span)

        for order in range(2):
            sr, si = outer((kin_s[order, 0, 0], kin_s[order, 0, 1]), True, split)
            spec_s[order, 0] = (by_real(sr, True) + by_imag(minus(si), True)) * (1.0 / length)
            dr, di = outer((kin_s[order, 1, 0], kin_s[order, 1, 1]), True, split)
            spec_s[order, 1] = (by_imag(dr, True) + by_real(di, True)) * (1.0 / length)
            if order == 0:
                serve_next(6)

    def short(ref, first):
        p = ref[...].astype(f32)
        lane = lax.broadcasted_iota(jnp.int32, (rows, span), 1)
        none = jnp.zeros((own, span), f32)
        back = pltpu.roll(p, 1, 1)
        back = jnp.where(lane == 0, jnp.concatenate([none, back[:-own]], axis=0), back)
        ahead = pltpu.roll(p, span - 1, 1)
        ahead = jnp.where(lane == span - 1, jnp.concatenate([ahead[own:], none], axis=0), ahead)
        tap = [cols_s[:, first + i : first + i + 1] for i in range(3)]
        return (back * tap[0] + p * tap[1] + ahead * tap[2]).astype(bf16)

    def convolve(order, values, signal, pieces):
        hr, hi = outer(values, False, pieces)
        xr = by_real(hr) + by_imag(minus(hi))
        xi = by_imag(hr) + by_real(hi)
        kr, ki = spec_s[order, 0], spec_s[order, 1]
        yr = pieces(xr * kr - xi * ki)
        yi = pieces(xr * ki + xi * kr)
        ur = by_real(yr) + by_imag(yi)
        ui = by_real(yi) + by_imag(minus(yr))
        tr, ti = tr_s[...], ti_s[...]
        wr = pieces(ur * tr + ui * ti)
        wi = pieces(ui * tr - ur * ti)
        y = signal * cols_s[:, 16 + order : 17 + order]
        for part in wr:
            y = y + dot(bwd_s[0:rows, 0:rows], part)
        for part in wi:
            y = y + dot(bwd_s[0:rows, rows : 2 * rows], part)
        return y

    prepare()

    @pl.loop(serve_base + 7, count)
    def _(to):
        serve(to)

    @pl.when(rank < turn_of_first)
    def _():
        serve(0)

    @pl.when(has_above)
    def _():
        edge(0).start()

    @pl.when(has_below)
    def _():
        edge(1).start()

    to_all(lambda to: remote(0, to, send_v, recv_v).wait_recv())
    pieces = split if DATA_PIECES == 2 else lambda x: (x.astype(bf16),)
    value = short(recv_v, 0)
    first_conv = convolve(0, (value,), value.astype(f32), pieces)
    to_all(lambda to: remote(1, to, send_a, recv_a).wait_recv())
    gated = short(recv_a, 8).astype(f32) * first_conv
    send_o[...] = convolve(1, pieces(gated), gated, pieces).astype(bf16)

    @pl.loop(0, count)
    def _(to):
        @pl.when(to != me)
        def _():
            remote(2, to, send_o, recv_o).start()

    recv_o[mine, :] = send_o[mine, :]

    @pl.when(has_above)
    def _():
        edge(0).wait_send()
        edge(1).wait_recv()

    @pl.when(has_below)
    def _():
        edge(1).wait_send()
        edge(0).wait_recv()

    gate = gate_s[...]
    row = lax.broadcasted_iota(jnp.int32, (span, share), 0)
    above = jnp.where(me == 0, 0.0, edge_recv[0])
    below = jnp.where(me == count - 1, 0.0, edge_recv[1])
    back = jnp.where(row == 0, above, pltpu.roll(gate, 1, 0))
    ahead = jnp.where(row == span - 1, below, pltpu.roll(gate, span - 1, 0))
    tap = taps_s[2].astype(f32)
    gate = (back * tap[0:1] + gate * tap[1:2] + ahead * tap[2:3]).astype(bf16).astype(f32)
    to_all(lambda to: remote(0, to, send_v, recv_v).wait_send())
    to_all(lambda to: remote(1, to, send_a, recv_a).wait_send())
    to_all(lambda to: remote(2, to, send_o, recv_o).wait_send())
    to_all(lambda to: remote(2, to, send_o, recv_o).wait_recv())
    out[...] = (gate * recv_o[...].astype(f32).T).astype(bf16)


def per_device(
    tokens,
    w_value,
    w_gate_a,
    w_gate_b,
    short_taps,
    pos_weight,
    pos_bias,
    sine_freq,
    hid_weight,
    hid_bias,
    filter_out,
    filter_bias,
    lag_decay,
):
    count = lax.axis_size("row")
    span, depth = tokens.shape
    share = w_value.shape[1]
    own = share // count
    rows = count * own
    hid = hid_weight.shape[0]
    feature_total = pos_weight.shape[0]
    forward, backward, turns, features = make_constants(count, own, span, feature_total)
    operands = [
        tokens,
        w_value,
        w_gate_a,
        w_gate_b,
        short_taps,
        pos_weight,
        pos_bias[None, :],
        sine_freq,
        hid_weight,
        hid_bias[None, :],
        filter_out,
        filter_bias,
        lag_decay[None, :],
        jnp.asarray(features),
        jnp.asarray(forward),
        jnp.asarray(backward),
        jnp.asarray(turns),
    ]
    cut = {4: (3, 3, share), 11: (2, share), 12: (1, share)}
    landing = [pltpu.VMEM(cut.get(i, x.shape), x.dtype) for i, x in enumerate(operands)]
    square = pltpu.VMEM((rows, span), bf16)
    scratch = [
        *landing,
        pltpu.VMEM((features.shape[0], hid), f32),
        pltpu.VMEM((24, hid), f32),
        pltpu.VMEM((32, share), f32),
        square,
        square,
        square,
        square,
        square,
        square,
        pltpu.VMEM((2, 1, share), f32),
        pltpu.VMEM((2, 1, share), f32),
        pltpu.VMEM((span, share), f32),
        pltpu.VMEM((rows, 32), f32),
        pltpu.VMEM((2, 2, 2, rows, span), bf16),
        pltpu.VMEM((2, 2, rows, span), f32),
        pltpu.VMEM((rows, span), f32),
        pltpu.VMEM((rows, span), f32),
        pltpu.SemaphoreType.REGULAR((count,)),
        pltpu.SemaphoreType.DMA((len(operands),)),
        pltpu.SemaphoreType.DMA((4, count)),
        pltpu.SemaphoreType.DMA((4, count)),
    ]
    return pl.pallas_call(
        functools.partial(kernel, count, own, hid, sine_coefficients()),
        out_shape=pltpu.VMEM((span, share), bf16),
        in_specs=[pl.BlockSpec(memory_space=pl.ANY)] * len(operands),
        out_specs=pl.BlockSpec(memory_space=pltpu.VMEM),
        scratch_shapes=scratch,
        compiler_params=pltpu.CompilerParams(collective_id=0, has_side_effects=True),
        name="gated_conv",
    )(*operands)


def solution(mesh):
    in_specs = (
        P(("grp", "row"), None),
        P(None, "col"),
        P(None, "col"),
        P(None, "col"),
        P(),
        P(),
        P(),
        P(),
        P(),
        P(),
        P(None, None, None, "col"),
        P(),
        P(),
    )
    out_specs = P(("grp", "row"), "col")
    return jax.shard_map(
        per_device, mesh=mesh, in_specs=in_specs, out_specs=out_specs, check_vma=False
    )
```

```python
import functools
import math

import jax
import jax.numpy as jnp
import numpy as np
from jax import lax
from jax.experimental import pallas as pl
from jax.experimental.pallas import tpu as pltpu
from jax.sharding import PartitionSpec as P

WINDOW_SHIFT = 0.05
MESH = pl.DeviceIdType.MESH
f32 = jnp.float32
bf16 = jnp.bfloat16
SIN_TERMS = 7


def sine_coefficients():
    nodes = 0.5 * np.cos((np.arange(400) + 0.5) * np.pi / 800)
    basis = np.polynomial.chebyshev.Chebyshev.fit(
        nodes * nodes, np.sin(2 * np.pi * nodes) / nodes, SIN_TERMS - 1, domain=[0, 0.25]
    )
    return [float(c) for c in basis.convert(kind=np.polynomial.Polynomial).coef]


def halves(values):
    high = values.astype(jnp.bfloat16)
    low = (values - high.astype(np.float32)).astype(jnp.bfloat16)
    return high, low


def make_constants(count, own, span, feature_total):
    length = count * span
    k1 = np.arange(count)[:, None] + 0.25
    outer = np.exp(2j * np.pi * k1 * np.arange(count)[None, :] / count)
    eye = np.eye(own)
    outer_rows = np.concatenate([np.kron(outer.real, eye), np.kron(outer.imag, eye)], axis=0)
    q = np.arange(span)
    inner = np.exp(2j * np.pi * (q[:, None] * q[None, :] % span) / span)
    turn = np.exp(2j * np.pi * k1 * q[None, :] / length)
    pieces = [*halves(outer_rows.astype(np.float32))]
    for part in (inner.real, inner.imag):
        pieces += [*halves(part.astype(np.float32))]
    forward = np.concatenate(pieces, axis=0)
    backward = np.concatenate([*halves(outer_rows.T.astype(np.float32))], axis=0)
    turns = np.concatenate([turn.real, turn.imag], axis=0).astype(np.float32)
    positions = np.arange(length, dtype=np.float64)
    bands = (feature_total - 1) // 2
    frequencies = np.linspace(1e-4, bands - 1, bands)
    angles = (2.0 * math.pi / length * positions)[None, :] * frequencies[:, None]
    features = np.concatenate(
        [positions[None, :] / max(length - 1, 1), np.cos(angles), -np.sin(angles)], axis=0
    )
    padded = -(-feature_total // 16) * 16
    table = np.zeros((padded, length), np.float32)
    table[:feature_total] = features
    return forward, backward, turns, np.concatenate([*halves(table)], axis=0)


def dot(a, b):
    return jnp.dot(a, b, preferred_element_type=f32)


def dot_nt(a, b):
    return lax.dot_general(a, b, (((1,), (1,)), ((), ())), preferred_element_type=f32)


def split(values):
    high = values.astype(bf16)
    return high, (values - high.astype(f32)).astype(bf16)


def pick(selector, table):
    high = table.astype(bf16)
    rest = table - high.astype(f32)
    middle = rest.astype(bf16)
    low = (rest - middle.astype(f32)).astype(bf16)
    return dot_nt(selector, high) + dot_nt(selector, middle) + dot_nt(selector, low)


def one_hot(rows, columns, first, own):
    row = lax.broadcasted_iota(jnp.int32, (rows, columns), 0)
    column = lax.broadcasted_iota(jnp.int32, (rows, columns), 1)
    return jnp.where(column == first + row % own, 1.0, 0.0).astype(bf16)


def sine_of_turns(turns, coefficients):
    u = turns - jnp.round(turns)
    square = u * u
    total = jnp.full_like(u, coefficients[-1])
    for c in coefficients[-2::-1]:
        total = total * square + c
    return total * u


def kernel(
    count,
    own,
    hid,
    coefficients,
    tokens,
    w_value,
    w_gate_a,
    w_gate_b,
    short_taps,
    pos_weight,
    pos_bias,
    sine_freq,
    hid_weight,
    hid_bias,
    filter_out,
    filter_bias,
    lag_decay,
    features,
    forward,
    backward,
    turns,
    out,
    tok_s,
    wv_s,
    wa_s,
    wb_s,
    taps_s,
    pw_s,
    pb_s,
    sf_s,
    hw_s,
    hb_s,
    fo_s,
    fb_s,
    ld_s,
    feat_s,
    fwd_s,
    bwd_s,
    turn_s,
    pw2_s,
    np_s,
    chan_s,
    send_v,
    recv_v,
    send_a,
    recv_a,
    send_o,
    recv_o,
    edge_send,
    edge_recv,
    gate_s,
    cols_s,
    kin_s,
    spec_s,
    tr_s,
    ti_s,
    ready_sem,
    local_sem,
    send_sem,
    recv_sem,
):
    me = lax.axis_index("row")
    col = lax.axis_index("col")
    span = tok_s.shape[0]
    share = wv_s.shape[1]
    length = count * span
    barrier = pltpu.get_barrier_semaphore()

    has_below = me > 0
    has_above = me < count - 1
    turn_of_first = max(count - 5, 0)

    def rank_of(place):
        return jnp.where(place == 0, turn_of_first, place - jnp.where(place <= turn_of_first, 1, 0))

    def place_of(turn):
        return jnp.where(turn == turn_of_first, 0, turn + jnp.where(turn < turn_of_first, 1, 0))

    rank = rank_of(me)

    def signal(semaphore, to):
        pl.semaphore_signal(semaphore, inc=1, device_id={"row": to}, device_id_type=MESH)

    start = pl.multiple_of(col * share, share)
    loads = [
        (tokens, tok_s),
        (w_value, wv_s),
        (w_gate_a, wa_s),
        (w_gate_b, wb_s),
        (short_taps.at[:, :, pl.ds(start, share)], taps_s),
        (pos_weight, pw_s),
        (pos_bias, pb_s),
        (sine_freq, sf_s),
        (hid_weight, hw_s),
        (hid_bias, hb_s),
        (filter_out, fo_s),
        (filter_bias.at[:, pl.ds(start, share)], fb_s),
        (lag_decay.at[:, pl.ds(start, share)], ld_s),
        (features, feat_s),
        (forward, fwd_s),
        (backward, bwd_s),
        (turns, turn_s),
    ]
    copies = [pltpu.make_async_copy(s, t, local_sem.at[i]) for i, (s, t) in enumerate(loads)]
    for c in copies[:3]:
        c.start()

    @pl.loop(rank + 1, count)
    def _(other):
        signal(barrier, place_of(other))

    @pl.when(rank > 0)
    def _():
        pl.semaphore_wait(barrier, rank)

    @pl.loop(0, rank)
    def _(other):
        signal(ready_sem.at[me], place_of(other))

    def remote(unit, to, source, target):
        d = lax.rem(to - me + count, count)
        return pltpu.make_async_remote_copy(
            src_ref=source.at[pl.ds(pl.multiple_of(to * own, own), own)],
            dst_ref=target.at[pl.ds(pl.multiple_of(me * own, own), own)],
            send_sem=send_sem.at[unit, d],
            recv_sem=recv_sem.at[unit, d],
            device_id={"row": to},
            device_id_type=MESH,
        )

    def to_all(body):
        @pl.loop(1, count)
        def _(d):
            body(lax.rem(me + d, count))

    copies[0].wait()
    copies[1].wait()
    for c in copies[3:]:
        c.start()
    mine = pl.ds(pl.multiple_of(me * own, own), own)

    def to_lower(unit, source, target):
        @pl.loop(0, count - 1)
        def _(i):
            step = lax.div(i + 1, 2)
            d = count // 2 + jnp.where(lax.rem(i, 2) == 1, step, -step)
            to = lax.rem(me + d, count)

            @pl.when(rank_of(to) < rank)
            def _():
                remote(unit, to, source, target).start()

        target[mine, :] = source[mine, :]

    send_v[...] = dot(tok_s[...], wv_s[...]).T.astype(bf16)
    to_lower(0, send_v, recv_v)
    copies[2].wait()
    send_a[...] = dot(tok_s[...], wa_s[...]).T.astype(bf16)
    to_lower(1, send_a, recv_a)

    def edge(side):
        return pltpu.make_async_remote_copy(
            src_ref=edge_send.at[side],
            dst_ref=edge_recv.at[side],
            send_sem=send_sem.at[3, side],
            recv_sem=recv_sem.at[3, side],
            device_id={"row": me + (1 if side == 0 else -1)},
            device_id_type=MESH,
        )

    rows = count * own
    two = 2 * rows
    outer_high, outer_low = fwd_s.at[0:two], fwd_s.at[two : 2 * two]
    at = 2 * two
    real_high, real_low = fwd_s.at[at : at + span], fwd_s.at[at + span : at + 2 * span]
    at = at + 2 * span
    imag_high, imag_low = fwd_s.at[at : at + span], fwd_s.at[at + span : at + 2 * span]

    def by(high, low, a, full):
        total = dot(a[0], high[...])
        if len(a) > 1:
            total = total + dot(a[1], high[...])
        if full:
            total = total + dot(a[0], low[...])
        return total

    def by_real(a, full=False):
        return by(real_high, real_low, a, full)

    def by_imag(a, full=False):
        return by(imag_high, imag_low, a, full)

    def minus(a):
        return tuple(-part for part in a)

    def outer(values, full, pieces):
        g = dot(outer_high[...], values[0])
        if len(values) > 1:
            g = g + dot(outer_high[...], values[1])
        if full:
            g = g + dot(outer_low[...], values[0])
        real, imag = g[:rows], g[rows:]
        tr, ti = tr_s[...], ti_s[...]
        return pieces(real * tr - imag * ti), pieces(real * ti + imag * tr)

    def serve(to):
        pl.semaphore_wait(ready_sem.at[to], 1)
        remote(0, to, send_v, recv_v).start()
        remote(1, to, send_a, recv_a).start()

    serve_base = jnp.where(me == 0, turn_of_first, me)

    def serve_next(steps):
        pl.when(serve_base + steps < count)(lambda: serve(serve_base + steps))

    def prepare():
        serve_next(1)
        serve_next(2)
        copies[3].wait()
        gate = dot(tok_s[...], wb_s[...]).astype(bf16).astype(f32)
        gate_s[...] = gate
        edge_send[0] = gate[span - 1 : span, :]
        edge_send[1] = gate[0:1, :]

        for c in copies[4:]:
            c.wait()

        chan_s[...] = jnp.zeros_like(chan_s)
        chan_s[0:3, :] = taps_s[0].astype(f32)
        chan_s[8:11, :] = taps_s[1].astype(f32)
        chan_s[16:18, :] = fb_s[...]
        chan_s[24:25, :] = ld_s[...]
        cols_s[...] = pick(one_hot(count * own, share, me * own, own), chan_s[...])
        hid_eye = one_hot(hid, hid, 0, hid)
        feature_total = pw_s.shape[0]
        padded = feat_s.shape[0] // 2
        pw2_s[...] = jnp.zeros_like(pw2_s)
        pw2_s[0:feature_total, :] = pw_s[...]
        pw2_s[padded : padded + feature_total, :] = pw_s[...]
        np_s[...] = jnp.zeros_like(np_s)
        np_s[0:2, :] = sf_s[...]
        np_s[8:9, :] = pb_s[...]
        np_s[16:17, :] = hb_s[...]
        net = pick(hid_eye, np_s[...])
        scale_a = net[:, 0:1] * (0.5 / math.pi)
        scale_b = net[:, 1:2] * (0.5 / math.pi)
        shift_a = net[:, 8:9] * scale_a
        shift_b = net[:, 16:17] * scale_b
        first_high, first_low = split(pick(hid_eye, pw2_s[...]))
        first_low = first_low[:, :padded]

        def three(table):
            high, low = split(table)
            lane = lax.broadcasted_iota(jnp.int32, table.shape, 1)
            return jnp.where(lane < 2 * hid, high.astype(f32), low.astype(f32)).astype(bf16)

        hw = hw_s[...]
        second = three(pick(hid_eye, jnp.concatenate([hw, hw, hw], axis=0)))
        own_hot = one_hot(own, share, me * own, own)
        weights = []
        for order in range(2):
            for side in range(2):
                w = fo_s[:, order, side, :]
                weights.append(pick(own_hot, jnp.concatenate([w, w, w], axis=0)))
        third = three(jnp.concatenate(weights, axis=0))
        decay = cols_s[0:own, 24:25]

        serve_next(3)

        blocks = 4
        width = length // blocks

        @pl.loop(0, blocks)
        def _(block):
            base = pl.multiple_of(block * width, width)
            feats = feat_s[:, pl.ds(base, width)]
            pre = dot(first_high, feats) + dot(first_low, feats[:padded])
            hidden = sine_of_turns(pre * scale_a + shift_a, coefficients)
            high, low = split(hidden)
            pre = dot(second, jnp.concatenate([high, low, high], axis=0))
            hidden = sine_of_turns(pre * scale_b + shift_b, coefficients)
            high, low = split(hidden)
            raw = dot(third, jnp.concatenate([high, low, high], axis=0))
            position = base + lax.broadcasted_iota(jnp.int32, (own, width), 1)
            scaled = position.astype(f32) * (1.0 / max(length - 1, 1))
            envelope = jnp.exp(-scaled * decay) + WINDOW_SHIFT
            later = jnp.where(position == 0, 0.0, envelope)
            for order in range(2):
                ahead = raw[2 * order * own : (2 * order + 1) * own] * envelope
                behind = raw[(2 * order + 1) * own : (2 * order + 2) * own] * later
                for kind, both in enumerate((ahead + behind, ahead - behind)):
                    high, low = split(both)
                    for part in range(width // span):
                        row = pl.multiple_of(block * (width // span) * own + part * own, own)
                        lanes = slice(part * span, (part + 1) * span)
                        kin_s[order, kind, 0, pl.ds(row, own), :] = high[:, lanes]
                        kin_s[order, kind, 1, pl.ds(row, own), :] = low[:, lanes]

            @pl.when(lax.rem(block, 2) == 1)
            def _():
                serve_next(4 + lax.div(block, 2))

        for part, target in enumerate((tr_s, ti_s)):
            one = turn_s[part * count : (part + 1) * count, :]
            target[...] = jnp.broadcast_to(one[:, None, :], (count, own, span)).reshape(rows, span)

        for order in range(2):
            sr, si = outer((kin_s[order, 0, 0], kin_s[order, 0, 1]), True, split)
            spec_s[order, 0] = (by_real(sr, True) + by_imag(minus(si), True)) * (1.0 / length)
            dr, di = outer((kin_s[order, 1, 0], kin_s[order, 1, 1]), True, split)
            spec_s[order, 1] = (by_imag(dr, True) + by_real(di, True)) * (1.0 / length)
            if order == 0:
                serve_next(6)

    def short(ref, first):
        p = ref[...].astype(f32)
        lane = lax.broadcasted_iota(jnp.int32, (rows, span), 1)
        none = jnp.zeros((own, span), f32)
        back = pltpu.roll(p, 1, 1)
        back = jnp.where(lane == 0, jnp.concatenate([none, back[:-own]], axis=0), back)
        ahead = pltpu.roll(p, span - 1, 1)
        ahead = jnp.where(lane == span - 1, jnp.concatenate([ahead[own:], none], axis=0), ahead)
        tap = [cols_s[:, first + i : first + i + 1] for i in range(3)]
        return (back * tap[0] + p * tap[1] + ahead * tap[2]).astype(bf16)

    def one(values):
        return (values.astype(bf16),)

    def convolve(order, values, signal):
        hr, hi = outer(values, False, one)
        xr = by_real(hr) + by_imag(minus(hi))
        xi = by_imag(hr) + by_real(hi)
        kr, ki = spec_s[order, 0], spec_s[order, 1]
        yr = one(xr * kr - xi * ki)
        yi = one(xr * ki + xi * kr)
        ur = by_real(yr) + by_imag(yi)
        ui = by_real(yi) + by_imag(minus(yr))
        tr, ti = tr_s[...], ti_s[...]
        wr = split(ur * tr + ui * ti)
        wi = split(ui * tr - ur * ti)
        y = signal * cols_s[:, 16 + order : 17 + order]
        for part in wr:
            y = y + dot(bwd_s[0:rows, 0:rows], part)
        for part in wi:
            y = y + dot(bwd_s[0:rows, rows : 2 * rows], part)
        return y

    prepare()

    @pl.loop(serve_base + 7, count)
    def _(to):
        serve(to)

    @pl.when(rank < turn_of_first)
    def _():
        serve(0)

    @pl.when(has_above)
    def _():
        edge(0).start()

    @pl.when(has_below)
    def _():
        edge(1).start()

    to_all(lambda to: remote(0, to, send_v, recv_v).wait_recv())
    value = short(recv_v, 0)
    first_conv = convolve(0, (value,), value.astype(f32))
    to_all(lambda to: remote(1, to, send_a, recv_a).wait_recv())
    gated = short(recv_a, 8).astype(f32) * first_conv
    send_o[...] = convolve(1, split(gated), gated).astype(bf16)

    @pl.loop(0, count)
    def _(to):
        @pl.when(to != me)
        def _():
            remote(2, to, send_o, recv_o).start()

    recv_o[mine, :] = send_o[mine, :]

    @pl.when(has_above)
    def _():
        edge(0).wait_send()
        edge(1).wait_recv()

    @pl.when(has_below)
    def _():
        edge(1).wait_send()
        edge(0).wait_recv()

    gate = gate_s[...]
    row = lax.broadcasted_iota(jnp.int32, (span, share), 0)
    above = jnp.where(me == 0, 0.0, edge_recv[0])
    below = jnp.where(me == count - 1, 0.0, edge_recv[1])
    back = jnp.where(row == 0, above, pltpu.roll(gate, 1, 0))
    ahead = jnp.where(row == span - 1, below, pltpu.roll(gate, span - 1, 0))
    tap = taps_s[2].astype(f32)
    gate = (back * tap[0:1] + gate * tap[1:2] + ahead * tap[2:3]).astype(bf16).astype(f32)
    to_all(lambda to: remote(0, to, send_v, recv_v).wait_send())
    to_all(lambda to: remote(1, to, send_a, recv_a).wait_send())
    to_all(lambda to: remote(2, to, send_o, recv_o).wait_send())
    to_all(lambda to: remote(2, to, send_o, recv_o).wait_recv())
    out[...] = (gate * recv_o[...].astype(f32).T).astype(bf16)


def per_device(
    tokens,
    w_value,
    w_gate_a,
    w_gate_b,
    short_taps,
    pos_weight,
    pos_bias,
    sine_freq,
    hid_weight,
    hid_bias,
    filter_out,
    filter_bias,
    lag_decay,
):
    count = lax.axis_size("row")
    span, depth = tokens.shape
    share = w_value.shape[1]
    own = share // count
    rows = count * own
    hid = hid_weight.shape[0]
    feature_total = pos_weight.shape[0]
    forward, backward, turns, features = make_constants(count, own, span, feature_total)
    operands = [
        tokens,
        w_value,
        w_gate_a,
        w_gate_b,
        short_taps,
        pos_weight,
        pos_bias[None, :],
        sine_freq,
        hid_weight,
        hid_bias[None, :],
        filter_out,
        filter_bias,
        lag_decay[None, :],
        jnp.asarray(features),
        jnp.asarray(forward),
        jnp.asarray(backward),
        jnp.asarray(turns),
    ]
    cut = {4: (3, 3, share), 11: (2, share), 12: (1, share)}
    landing = [pltpu.VMEM(cut.get(i, x.shape), x.dtype) for i, x in enumerate(operands)]
    square = pltpu.VMEM((rows, span), bf16)
    scratch = [
        *landing,
        pltpu.VMEM((features.shape[0], hid), f32),
        pltpu.VMEM((24, hid), f32),
        pltpu.VMEM((32, share), f32),
        square,
        square,
        square,
        square,
        square,
        square,
        pltpu.VMEM((2, 1, share), f32),
        pltpu.VMEM((2, 1, share), f32),
        pltpu.VMEM((span, share), f32),
        pltpu.VMEM((rows, 32), f32),
        pltpu.VMEM((2, 2, 2, rows, span), bf16),
        pltpu.VMEM((2, 2, rows, span), f32),
        pltpu.VMEM((rows, span), f32),
        pltpu.VMEM((rows, span), f32),
        pltpu.SemaphoreType.REGULAR((count,)),
        pltpu.SemaphoreType.DMA((len(operands),)),
        pltpu.SemaphoreType.DMA((4, count)),
        pltpu.SemaphoreType.DMA((4, count)),
    ]
    return pl.pallas_call(
        functools.partial(kernel, count, own, hid, sine_coefficients()),
        out_shape=pltpu.VMEM((span, share), bf16),
        in_specs=[pl.BlockSpec(memory_space=pl.ANY)] * len(operands),
        out_specs=pl.BlockSpec(memory_space=pltpu.VMEM),
        scratch_shapes=scratch,
        compiler_params=pltpu.CompilerParams(collective_id=0, has_side_effects=True),
        name="gated_conv",
    )(*operands)


def solution(mesh):
    in_specs = (
        P(("grp", "row"), None),
        P(None, "col"),
        P(None, "col"),
        P(None, "col"),
        P(),
        P(),
        P(),
        P(),
        P(),
        P(),
        P(None, None, None, "col"),
        P(),
        P(),
    )
    out_specs = P(("grp", "row"), "col")
    return jax.shard_map(
        per_device, mesh=mesh, in_specs=in_specs, out_specs=out_specs, check_vma=False
    )
```

```python
import functools
import math

import jax
import jax.numpy as jnp
import numpy as np
from jax import lax
from jax.experimental import pallas as pl
from jax.experimental.pallas import tpu as pltpu
from jax.sharding import PartitionSpec as P

WINDOW_SHIFT = 0.05
MESH = pl.DeviceIdType.MESH
f32 = jnp.float32
bf16 = jnp.bfloat16
SIN_TERMS = 7


def sine_coefficients():
    nodes = 0.5 * np.cos((np.arange(400) + 0.5) * np.pi / 800)
    basis = np.polynomial.chebyshev.Chebyshev.fit(
        nodes * nodes, np.sin(2 * np.pi * nodes) / nodes, SIN_TERMS - 1, domain=[0, 0.25]
    )
    return [float(c) for c in basis.convert(kind=np.polynomial.Polynomial).coef]


def halves(values):
    high = values.astype(jnp.bfloat16)
    low = (values - high.astype(np.float32)).astype(jnp.bfloat16)
    return high, low


def make_constants(count, own, span, feature_total):
    length = count * span
    k1 = np.arange(count)[:, None] + 0.25
    outer = np.exp(2j * np.pi * k1 * np.arange(count)[None, :] / count)
    eye = np.eye(own)
    outer_rows = np.concatenate([np.kron(outer.real, eye), np.kron(outer.imag, eye)], axis=0)
    q = np.arange(span)
    inner = np.exp(2j * np.pi * (q[:, None] * q[None, :] % span) / span)
    turn = np.exp(2j * np.pi * k1 * q[None, :] / length)
    pieces = [*halves(outer_rows.astype(np.float32))]
    for part in (inner.real, inner.imag):
        pieces += [*halves(part.astype(np.float32))]
    forward = np.concatenate(pieces, axis=0)
    backward = np.concatenate([*halves(outer_rows.T.astype(np.float32))], axis=0)
    turns = np.concatenate([turn.real, turn.imag], axis=0).astype(np.float32)
    positions = np.arange(length, dtype=np.float64)
    bands = (feature_total - 1) // 2
    frequencies = np.linspace(1e-4, bands - 1, bands)
    angles = (2.0 * math.pi / length * positions)[None, :] * frequencies[:, None]
    features = np.concatenate(
        [positions[None, :] / max(length - 1, 1), np.cos(angles), -np.sin(angles)], axis=0
    )
    padded = -(-feature_total // 16) * 16
    table = np.zeros((padded, length), np.float32)
    table[:feature_total] = features
    return forward, backward, turns, np.concatenate([*halves(table)], axis=0)


def dot(a, b):
    return jnp.dot(a, b, preferred_element_type=f32)


def dot_nt(a, b):
    return lax.dot_general(a, b, (((1,), (1,)), ((), ())), preferred_element_type=f32)


def split(values):
    high = values.astype(bf16)
    return high, (values - high.astype(f32)).astype(bf16)


def pick(selector, table):
    high = table.astype(bf16)
    rest = table - high.astype(f32)
    middle = rest.astype(bf16)
    low = (rest - middle.astype(f32)).astype(bf16)
    return dot_nt(selector, high) + dot_nt(selector, middle) + dot_nt(selector, low)


def one_hot(rows, columns, first, own):
    row = lax.broadcasted_iota(jnp.int32, (rows, columns), 0)
    column = lax.broadcasted_iota(jnp.int32, (rows, columns), 1)
    return jnp.where(column == first + row % own, 1.0, 0.0).astype(bf16)


def sine_of_turns(turns, coefficients):
    u = turns - jnp.round(turns)
    square = u * u
    total = jnp.full_like(u, coefficients[-1])
    for c in coefficients[-2::-1]:
        total = total * square + c
    return total * u


def kernel(
    count,
    own,
    hid,
    coefficients,
    tokens,
    w_value,
    w_gate_a,
    w_gate_b,
    short_taps,
    pos_weight,
    pos_bias,
    sine_freq,
    hid_weight,
    hid_bias,
    filter_out,
    filter_bias,
    lag_decay,
    features,
    forward,
    backward,
    turns,
    out,
    tok_s,
    wv_s,
    wa_s,
    wb_s,
    taps_s,
    pw_s,
    pb_s,
    sf_s,
    hw_s,
    hb_s,
    fo_s,
    fb_s,
    ld_s,
    feat_s,
    fwd_s,
    bwd_s,
    turn_s,
    pw2_s,
    np_s,
    chan_s,
    send_v,
    recv_v,
    send_a,
    recv_a,
    send_o,
    recv_o,
    edge_send,
    edge_recv,
    gate_s,
    cols_s,
    kin_s,
    spec_s,
    tr_s,
    ti_s,
    ready_sem,
    local_sem,
    send_sem,
    recv_sem,
):
    me = lax.axis_index("row")
    col = lax.axis_index("col")
    span = tok_s.shape[0]
    share = wv_s.shape[1]
    length = count * span
    barrier = pltpu.get_barrier_semaphore()

    has_below = me > 0
    has_above = me < count - 1
    turn_of_first = max(count - 7, 0)

    def rank_of(place):
        return jnp.where(place == 0, turn_of_first, place - jnp.where(place <= turn_of_first, 1, 0))

    def place_of(turn):
        return jnp.where(turn == turn_of_first, 0, turn + jnp.where(turn < turn_of_first, 1, 0))

    rank = rank_of(me)

    def signal(semaphore, to):
        pl.semaphore_signal(semaphore, inc=1, device_id={"row": to}, device_id_type=MESH)

    start = pl.multiple_of(col * share, share)
    loads = [
        (tokens, tok_s),
        (w_value, wv_s),
        (w_gate_a, wa_s),
        (w_gate_b, wb_s),
        (short_taps.at[:, :, pl.ds(start, share)], taps_s),
        (pos_weight, pw_s),
        (pos_bias, pb_s),
        (sine_freq, sf_s),
        (hid_weight, hw_s),
        (hid_bias, hb_s),
        (filter_out, fo_s),
        (filter_bias.at[:, pl.ds(start, share)], fb_s),
        (lag_decay.at[:, pl.ds(start, share)], ld_s),
        (features, feat_s),
        (forward, fwd_s),
        (backward, bwd_s),
        (turns, turn_s),
    ]
    copies = [pltpu.make_async_copy(s, t, local_sem.at[i]) for i, (s, t) in enumerate(loads)]
    for c in copies[:3]:
        c.start()

    @pl.loop(rank + 1, count)
    def _(other):
        signal(barrier, place_of(other))

    @pl.when(rank > 0)
    def _():
        pl.semaphore_wait(barrier, rank)

    @pl.loop(0, rank)
    def _(other):
        signal(ready_sem.at[me], place_of(other))

    def remote(unit, to, source, target):
        d = lax.rem(to - me + count, count)
        return pltpu.make_async_remote_copy(
            src_ref=source.at[pl.ds(pl.multiple_of(to * own, own), own)],
            dst_ref=target.at[pl.ds(pl.multiple_of(me * own, own), own)],
            send_sem=send_sem.at[unit, d],
            recv_sem=recv_sem.at[unit, d],
            device_id={"row": to},
            device_id_type=MESH,
        )

    def to_all(body):
        @pl.loop(1, count)
        def _(d):
            body(lax.rem(me + d, count))

    copies[0].wait()
    copies[1].wait()
    for c in copies[3:]:
        c.start()
    mine = pl.ds(pl.multiple_of(me * own, own), own)

    def to_lower(unit, source, target):
        @pl.loop(0, count - 1)
        def _(i):
            step = lax.div(i + 1, 2)
            d = count // 2 + jnp.where(lax.rem(i, 2) == 1, step, -step)
            to = lax.rem(me + d, count)

            @pl.when(rank_of(to) < rank)
            def _():
                remote(unit, to, source, target).start()

        target[mine, :] = source[mine, :]

    send_v[...] = dot(tok_s[...], wv_s[...]).T.astype(bf16)
    to_lower(0, send_v, recv_v)
    copies[2].wait()
    send_a[...] = dot(tok_s[...], wa_s[...]).T.astype(bf16)
    to_lower(1, send_a, recv_a)

    def edge(side):
        return pltpu.make_async_remote_copy(
            src_ref=edge_send.at[side],
            dst_ref=edge_recv.at[side],
            send_sem=send_sem.at[3, side],
            recv_sem=recv_sem.at[3, side],
            device_id={"row": me + (1 if side == 0 else -1)},
            device_id_type=MESH,
        )

    rows = count * own
    two = 2 * rows
    outer_high, outer_low = fwd_s.at[0:two], fwd_s.at[two : 2 * two]
    at = 2 * two
    real_high, real_low = fwd_s.at[at : at + span], fwd_s.at[at + span : at + 2 * span]
    at = at + 2 * span
    imag_high, imag_low = fwd_s.at[at : at + span], fwd_s.at[at + span : at + 2 * span]

    def by(high, low, a, full):
        total = dot(a[0], high[...])
        if len(a) > 1:
            total = total + dot(a[1], high[...])
        if full:
            total = total + dot(a[0], low[...])
        return total

    def by_real(a, full=False):
        return by(real_high, real_low, a, full)

    def by_imag(a, full=False):
        return by(imag_high, imag_low, a, full)

    def minus(a):
        return tuple(-part for part in a)

    def outer(values, full, pieces):
        g = dot(outer_high[...], values[0])
        if len(values) > 1:
            g = g + dot(outer_high[...], values[1])
        if full:
            g = g + dot(outer_low[...], values[0])
        real, imag = g[:rows], g[rows:]
        tr, ti = tr_s[...], ti_s[...]
        return pieces(real * tr - imag * ti), pieces(real * ti + imag * tr)

    def serve(to):
        pl.semaphore_wait(ready_sem.at[to], 1)
        remote(0, to, send_v, recv_v).start()
        remote(1, to, send_a, recv_a).start()

    serve_base = jnp.where(me == 0, turn_of_first, me)

    def serve_next(steps):
        pl.when(serve_base + steps < count)(lambda: serve(serve_base + steps))

    def serve_rest(steps):
        @pl.loop(serve_base + steps, count)
        def _(to):
            serve(to)

        @pl.when(rank < turn_of_first)
        def _():
            serve(0)

    def prepare():
        serve_next(1)
        serve_next(2)
        copies[3].wait()
        gate = dot(tok_s[...], wb_s[...]).astype(bf16).astype(f32)
        gate_s[...] = gate
        edge_send[0] = gate[span - 1 : span, :]
        edge_send[1] = gate[0:1, :]

        for c in copies[4:]:
            c.wait()

        chan_s[...] = jnp.zeros_like(chan_s)
        chan_s[0:3, :] = taps_s[0].astype(f32)
        chan_s[8:11, :] = taps_s[1].astype(f32)
        chan_s[16:18, :] = fb_s[...]
        chan_s[24:25, :] = ld_s[...]
        cols_s[...] = pick(one_hot(count * own, share, me * own, own), chan_s[...])
        hid_eye = one_hot(hid, hid, 0, hid)
        feature_total = pw_s.shape[0]
        padded = feat_s.shape[0] // 2
        pw2_s[...] = jnp.zeros_like(pw2_s)
        pw2_s[0:feature_total, :] = pw_s[...]
        pw2_s[padded : padded + feature_total, :] = pw_s[...]
        np_s[...] = jnp.zeros_like(np_s)
        np_s[0:2, :] = sf_s[...]
        np_s[8:9, :] = pb_s[...]
        np_s[16:17, :] = hb_s[...]
        net = pick(hid_eye, np_s[...])
        scale_a = net[:, 0:1] * (0.5 / math.pi)
        scale_b = net[:, 1:2] * (0.5 / math.pi)
        shift_a = net[:, 8:9] * scale_a
        shift_b = net[:, 16:17] * scale_b
        first_high, first_low = split(pick(hid_eye, pw2_s[...]))
        first_low = first_low[:, :padded]

        def three(table):
            high, low = split(table)
            lane = lax.broadcasted_iota(jnp.int32, table.shape, 1)
            return jnp.where(lane < 2 * hid, high.astype(f32), low.astype(f32)).astype(bf16)

        hw = hw_s[...]
        second = three(pick(hid_eye, jnp.concatenate([hw, hw, hw], axis=0)))
        own_hot = one_hot(own, share, me * own, own)
        weights = []
        for order in range(2):
            for side in range(2):
                w = fo_s[:, order, side, :]
                weights.append(pick(own_hot, jnp.concatenate([w, w, w], axis=0)))
        third = three(jnp.concatenate(weights, axis=0))
        decay = cols_s[0:own, 24:25]

        serve_next(3)

        blocks = 4
        width = length // blocks

        @pl.loop(0, blocks)
        def _(block):
            base = pl.multiple_of(block * width, width)
            feats = feat_s[:, pl.ds(base, width)]
            pre = dot(first_high, feats) + dot(first_low, feats[:padded])
            hidden = sine_of_turns(pre * scale_a + shift_a, coefficients)
            high, low = split(hidden)
            pre = dot(second, jnp.concatenate([high, low, high], axis=0))
            hidden = sine_of_turns(pre * scale_b + shift_b, coefficients)
            high, low = split(hidden)
            raw = dot(third, jnp.concatenate([high, low, high], axis=0))
            position = base + lax.broadcasted_iota(jnp.int32, (own, width), 1)
            scaled = position.astype(f32) * (1.0 / max(length - 1, 1))
            envelope = jnp.exp(-scaled * decay) + WINDOW_SHIFT
            later = jnp.where(position == 0, 0.0, envelope)
            for order in range(2):
                ahead = raw[2 * order * own : (2 * order + 1) * own] * envelope
                behind = raw[(2 * order + 1) * own : (2 * order + 2) * own] * later
                for kind, both in enumerate((ahead + behind, ahead - behind)):
                    high, low = split(both)
                    for part in range(width // span):
                        row = pl.multiple_of(block * (width // span) * own + part * own, own)
                        lanes = slice(part * span, (part + 1) * span)
                        kin_s[order, kind, 0, pl.ds(row, own), :] = high[:, lanes]
                        kin_s[order, kind, 1, pl.ds(row, own), :] = low[:, lanes]

            @pl.when(lax.rem(block, 2) == 1)
            def _():
                serve_next(4 + lax.div(block, 2))

        for part, target in enumerate((tr_s, ti_s)):
            one = turn_s[part * count : (part + 1) * count, :]
            target[...] = jnp.broadcast_to(one[:, None, :], (count, own, span)).reshape(rows, span)

        for order in range(2):
            sr, si = outer((kin_s[order, 0, 0], kin_s[order, 0, 1]), True, split)
            spec_s[order, 0] = (by_real(sr, True) + by_imag(minus(si), True)) * (1.0 / length)
            dr, di = outer((kin_s[order, 1, 0], kin_s[order, 1, 1]), True, split)
            spec_s[order, 1] = (by_imag(dr, True) + by_real(di, True)) * (1.0 / length)
            if order == 0:
                serve_rest(6)

    def short(ref, first):
        p = ref[...].astype(f32)
        lane = lax.broadcasted_iota(jnp.int32, (rows, span), 1)
        none = jnp.zeros((own, span), f32)
        back = pltpu.roll(p, 1, 1)
        back = jnp.where(lane == 0, jnp.concatenate([none, back[:-own]], axis=0), back)
        ahead = pltpu.roll(p, span - 1, 1)
        ahead = jnp.where(lane == span - 1, jnp.concatenate([ahead[own:], none], axis=0), ahead)
        tap = [cols_s[:, first + i : first + i + 1] for i in range(3)]
        return (back * tap[0] + p * tap[1] + ahead * tap[2]).astype(bf16)

    def one(values):
        return (values.astype(bf16),)

    def convolve(order, values, signal):
        hr, hi = outer(values, False, one)
        xr = by_real(hr) + by_imag(minus(hi))
        xi = by_imag(hr) + by_real(hi)
        kr, ki = spec_s[order, 0], spec_s[order, 1]
        yr = one(xr * kr - xi * ki)
        yi = one(xr * ki + xi * kr)
        ur = by_real(yr) + by_imag(yi)
        ui = by_real(yi) + by_imag(minus(yr))
        tr, ti = tr_s[...], ti_s[...]
        wr = split(ur * tr + ui * ti)
        wi = split(ui * tr - ur * ti)
        y = signal * cols_s[:, 16 + order : 17 + order]
        for part in wr:
            y = y + dot(bwd_s[0:rows, 0:rows], part)
        for part in wi:
            y = y + dot(bwd_s[0:rows, rows : 2 * rows], part)
        return y

    prepare()

    @pl.when(has_above)
    def _():
        edge(0).start()

    @pl.when(has_below)
    def _():
        edge(1).start()

    to_all(lambda to: remote(0, to, send_v, recv_v).wait_recv())
    value = short(recv_v, 0)
    first_conv = convolve(0, (value,), value.astype(f32))
    to_all(lambda to: remote(1, to, send_a, recv_a).wait_recv())
    gated = short(recv_a, 8).astype(f32) * first_conv
    send_o[...] = convolve(1, split(gated), gated).astype(bf16)

    @pl.loop(0, count)
    def _(to):
        @pl.when(to != me)
        def _():
            remote(2, to, send_o, recv_o).start()

    recv_o[mine, :] = send_o[mine, :]

    @pl.when(has_above)
    def _():
        edge(0).wait_send()
        edge(1).wait_recv()

    @pl.when(has_below)
    def _():
        edge(1).wait_send()
        edge(0).wait_recv()

    gate = gate_s[...]
    row = lax.broadcasted_iota(jnp.int32, (span, share), 0)
    above = jnp.where(me == 0, 0.0, edge_recv[0])
    below = jnp.where(me == count - 1, 0.0, edge_recv[1])
    back = jnp.where(row == 0, above, pltpu.roll(gate, 1, 0))
    ahead = jnp.where(row == span - 1, below, pltpu.roll(gate, span - 1, 0))
    tap = taps_s[2].astype(f32)
    gate = (back * tap[0:1] + gate * tap[1:2] + ahead * tap[2:3]).astype(bf16).astype(f32)
    to_all(lambda to: remote(0, to, send_v, recv_v).wait_send())
    to_all(lambda to: remote(1, to, send_a, recv_a).wait_send())
    to_all(lambda to: remote(2, to, send_o, recv_o).wait_send())
    to_all(lambda to: remote(2, to, send_o, recv_o).wait_recv())
    out[...] = (gate * recv_o[...].astype(f32).T).astype(bf16)


def per_device(
    tokens,
    w_value,
    w_gate_a,
    w_gate_b,
    short_taps,
    pos_weight,
    pos_bias,
    sine_freq,
    hid_weight,
    hid_bias,
    filter_out,
    filter_bias,
    lag_decay,
):
    count = lax.axis_size("row")
    span, depth = tokens.shape
    share = w_value.shape[1]
    own = share // count
    rows = count * own
    hid = hid_weight.shape[0]
    feature_total = pos_weight.shape[0]
    forward, backward, turns, features = make_constants(count, own, span, feature_total)
    operands = [
        tokens,
        w_value,
        w_gate_a,
        w_gate_b,
        short_taps,
        pos_weight,
        pos_bias[None, :],
        sine_freq,
        hid_weight,
        hid_bias[None, :],
        filter_out,
        filter_bias,
        lag_decay[None, :],
        jnp.asarray(features),
        jnp.asarray(forward),
        jnp.asarray(backward),
        jnp.asarray(turns),
    ]
    cut = {4: (3, 3, share), 11: (2, share), 12: (1, share)}
    landing = [pltpu.VMEM(cut.get(i, x.shape), x.dtype) for i, x in enumerate(operands)]
    square = pltpu.VMEM((rows, span), bf16)
    scratch = [
        *landing,
        pltpu.VMEM((features.shape[0], hid), f32),
        pltpu.VMEM((24, hid), f32),
        pltpu.VMEM((32, share), f32),
        square,
        square,
        square,
        square,
        square,
        square,
        pltpu.VMEM((2, 1, share), f32),
        pltpu.VMEM((2, 1, share), f32),
        pltpu.VMEM((span, share), f32),
        pltpu.VMEM((rows, 32), f32),
        pltpu.VMEM((2, 2, 2, rows, span), bf16),
        pltpu.VMEM((2, 2, rows, span), f32),
        pltpu.VMEM((rows, span), f32),
        pltpu.VMEM((rows, span), f32),
        pltpu.SemaphoreType.REGULAR((count,)),
        pltpu.SemaphoreType.DMA((len(operands),)),
        pltpu.SemaphoreType.DMA((4, count)),
        pltpu.SemaphoreType.DMA((4, count)),
    ]
    return pl.pallas_call(
        functools.partial(kernel, count, own, hid, sine_coefficients()),
        out_shape=pltpu.VMEM((span, share), bf16),
        in_specs=[pl.BlockSpec(memory_space=pl.ANY)] * len(operands),
        out_specs=pl.BlockSpec(memory_space=pltpu.VMEM),
        scratch_shapes=scratch,
        compiler_params=pltpu.CompilerParams(collective_id=0, has_side_effects=True),
        name="gated_conv",
    )(*operands)


def solution(mesh):
    in_specs = (
        P(("grp", "row"), None),
        P(None, "col"),
        P(None, "col"),
        P(None, "col"),
        P(),
        P(),
        P(),
        P(),
        P(),
        P(),
        P(None, None, None, "col"),
        P(),
        P(),
    )
    out_specs = P(("grp", "row"), "col")
    return jax.shard_map(
        per_device, mesh=mesh, in_specs=in_specs, out_specs=out_specs, check_vma=False
    )
```

```python
import functools
import math

import jax
import jax.numpy as jnp
import numpy as np
from jax import lax
from jax.experimental import pallas as pl
from jax.experimental.pallas import tpu as pltpu
from jax.sharding import PartitionSpec as P

WINDOW_SHIFT = 0.05
MESH = pl.DeviceIdType.MESH
f32 = jnp.float32
bf16 = jnp.bfloat16
SIN_TERMS = 7


def sine_coefficients():
    nodes = 0.5 * np.cos((np.arange(400) + 0.5) * np.pi / 800)
    basis = np.polynomial.chebyshev.Chebyshev.fit(
        nodes * nodes, np.sin(2 * np.pi * nodes) / nodes, SIN_TERMS - 1, domain=[0, 0.25]
    )
    return [float(c) for c in basis.convert(kind=np.polynomial.Polynomial).coef]


def halves(values):
    high = values.astype(jnp.bfloat16)
    low = (values - high.astype(np.float32)).astype(jnp.bfloat16)
    return high, low


def make_constants(count, own, span, feature_total):
    length = count * span
    k1 = np.arange(count)[:, None] + 0.25
    outer = np.exp(2j * np.pi * k1 * np.arange(count)[None, :] / count)
    eye = np.eye(own)
    outer_rows = np.concatenate([np.kron(outer.real, eye), np.kron(outer.imag, eye)], axis=0)
    q = np.arange(span)
    inner = np.exp(2j * np.pi * (q[:, None] * q[None, :] % span) / span)
    turn = np.exp(2j * np.pi * k1 * q[None, :] / length)
    pieces = [*halves(outer_rows.astype(np.float32))]
    for part in (inner.real, inner.imag):
        pieces += [*halves(part.astype(np.float32))]
    forward = np.concatenate(pieces, axis=0)
    backward = np.concatenate([*halves(outer_rows.T.astype(np.float32))], axis=0)
    turns = np.concatenate([turn.real, turn.imag], axis=0).astype(np.float32)
    positions = np.arange(length, dtype=np.float64)
    bands = (feature_total - 1) // 2
    frequencies = np.linspace(1e-4, bands - 1, bands)
    angles = (2.0 * math.pi / length * positions)[None, :] * frequencies[:, None]
    features = np.concatenate(
        [positions[None, :] / max(length - 1, 1), np.cos(angles), -np.sin(angles)], axis=0
    )
    padded = -(-feature_total // 16) * 16
    table = np.zeros((padded, length), np.float32)
    table[:feature_total] = features
    return forward, backward, turns, np.concatenate([*halves(table)], axis=0)


def dot(a, b):
    return jnp.dot(a, b, preferred_element_type=f32)


def dot_nt(a, b):
    return lax.dot_general(a, b, (((1,), (1,)), ((), ())), preferred_element_type=f32)


def split(values):
    high = values.astype(bf16)
    return high, (values - high.astype(f32)).astype(bf16)


def pick(selector, table):
    high = table.astype(bf16)
    rest = table - high.astype(f32)
    middle = rest.astype(bf16)
    low = (rest - middle.astype(f32)).astype(bf16)
    return dot_nt(selector, high) + dot_nt(selector, middle) + dot_nt(selector, low)


def one_hot(rows, columns, first, own):
    row = lax.broadcasted_iota(jnp.int32, (rows, columns), 0)
    column = lax.broadcasted_iota(jnp.int32, (rows, columns), 1)
    return jnp.where(column == first + row % own, 1.0, 0.0).astype(bf16)


def sine_of_turns(turns, coefficients):
    u = turns - jnp.round(turns)
    square = u * u
    total = jnp.full_like(u, coefficients[-1])
    for c in coefficients[-2::-1]:
        total = total * square + c
    return total * u


def kernel(
    count,
    own,
    hid,
    coefficients,
    tokens,
    w_value,
    w_gate_a,
    w_gate_b,
    short_taps,
    pos_weight,
    pos_bias,
    sine_freq,
    hid_weight,
    hid_bias,
    filter_out,
    filter_bias,
    lag_decay,
    features,
    forward,
    backward,
    turns,
    out,
    tok_s,
    wv_s,
    wa_s,
    wb_s,
    taps_s,
    pw_s,
    pb_s,
    sf_s,
    hw_s,
    hb_s,
    fo_s,
    fb_s,
    ld_s,
    feat_s,
    fwd_s,
    bwd_s,
    turn_s,
    pw2_s,
    np_s,
    chan_s,
    send_v,
    recv_v,
    send_a,
    recv_a,
    send_o,
    recv_o,
    edge_send,
    edge_recv,
    gate_s,
    cols_s,
    kin_s,
    spec_s,
    tr_s,
    ti_s,
    ready_sem,
    local_sem,
    send_sem,
    recv_sem,
):
    me = lax.axis_index("row")
    col = lax.axis_index("col")
    span = tok_s.shape[0]
    share = wv_s.shape[1]
    length = count * span
    barrier = pltpu.get_barrier_semaphore()

    has_below = me > 0
    has_above = me < count - 1
    turn_of_first = max(count - 8, 0)

    def rank_of(place):
        return jnp.where(place == 0, turn_of_first, place - jnp.where(place <= turn_of_first, 1, 0))

    def place_of(turn):
        return jnp.where(turn == turn_of_first, 0, turn + jnp.where(turn < turn_of_first, 1, 0))

    rank = rank_of(me)

    def signal(semaphore, to):
        pl.semaphore_signal(semaphore, inc=1, device_id={"row": to}, device_id_type=MESH)

    start = pl.multiple_of(col * share, share)
    loads = [
        (tokens, tok_s),
        (w_value, wv_s),
        (w_gate_a, wa_s),
        (w_gate_b, wb_s),
        (short_taps.at[:, :, pl.ds(start, share)], taps_s),
        (pos_weight, pw_s),
        (pos_bias, pb_s),
        (sine_freq, sf_s),
        (hid_weight, hw_s),
        (hid_bias, hb_s),
        (filter_out, fo_s),
        (filter_bias.at[:, pl.ds(start, share)], fb_s),
        (lag_decay.at[:, pl.ds(start, share)], ld_s),
        (features, feat_s),
        (forward, fwd_s),
        (backward, bwd_s),
        (turns, turn_s),
    ]
    copies = [pltpu.make_async_copy(s, t, local_sem.at[i]) for i, (s, t) in enumerate(loads)]
    for c in copies[:3]:
        c.start()

    @pl.loop(rank + 1, count)
    def _(other):
        signal(barrier, place_of(other))

    @pl.when(rank > 0)
    def _():
        pl.semaphore_wait(barrier, rank)

    @pl.loop(0, rank)
    def _(other):
        signal(ready_sem.at[me], place_of(other))

    def remote(unit, to, source, target):
        d = lax.rem(to - me + count, count)
        return pltpu.make_async_remote_copy(
            src_ref=source.at[pl.ds(pl.multiple_of(to * own, own), own)],
            dst_ref=target.at[pl.ds(pl.multiple_of(me * own, own), own)],
            send_sem=send_sem.at[unit, d],
            recv_sem=recv_sem.at[unit, d],
            device_id={"row": to},
            device_id_type=MESH,
        )

    def to_all(body):
        @pl.loop(1, count)
        def _(d):
            body(lax.rem(me + d, count))

    copies[0].wait()
    copies[1].wait()
    for c in copies[3:]:
        c.start()
    mine = pl.ds(pl.multiple_of(me * own, own), own)

    def to_lower(unit, source, target):
        @pl.loop(0, count - 1)
        def _(i):
            step = lax.div(i + 1, 2)
            d = count // 2 + jnp.where(lax.rem(i, 2) == 1, step, -step)
            to = lax.rem(me + d, count)

            @pl.when(rank_of(to) < rank)
            def _():
                remote(unit, to, source, target).start()

        target[mine, :] = source[mine, :]

    send_v[...] = dot(tok_s[...], wv_s[...]).T.astype(bf16)
    to_lower(0, send_v, recv_v)
    copies[2].wait()
    send_a[...] = dot(tok_s[...], wa_s[...]).T.astype(bf16)
    to_lower(1, send_a, recv_a)

    def edge(side):
        return pltpu.make_async_remote_copy(
            src_ref=edge_send.at[side],
            dst_ref=edge_recv.at[side],
            send_sem=send_sem.at[3, side],
            recv_sem=recv_sem.at[3, side],
            device_id={"row": me + (1 if side == 0 else -1)},
            device_id_type=MESH,
        )

    rows = count * own
    two = 2 * rows
    outer_high, outer_low = fwd_s.at[0:two], fwd_s.at[two : 2 * two]
    at = 2 * two
    real_high, real_low = fwd_s.at[at : at + span], fwd_s.at[at + span : at + 2 * span]
    at = at + 2 * span
    imag_high, imag_low = fwd_s.at[at : at + span], fwd_s.at[at + span : at + 2 * span]

    def by(high, low, a, full):
        total = dot(a[0], high[...])
        if len(a) > 1:
            total = total + dot(a[1], high[...])
        if full:
            total = total + dot(a[0], low[...])
        return total

    def by_real(a, full=False):
        return by(real_high, real_low, a, full)

    def by_imag(a, full=False):
        return by(imag_high, imag_low, a, full)

    def minus(a):
        return tuple(-part for part in a)

    def outer(values, full, pieces):
        g = dot(outer_high[...], values[0])
        if len(values) > 1:
            g = g + dot(outer_high[...], values[1])
        if full:
            g = g + dot(outer_low[...], values[0])
        real, imag = g[:rows], g[rows:]
        tr, ti = tr_s[...], ti_s[...]
        return pieces(real * tr - imag * ti), pieces(real * ti + imag * tr)

    def serve(to):
        pl.semaphore_wait(ready_sem.at[to], 1)
        remote(0, to, send_v, recv_v).start()
        remote(1, to, send_a, recv_a).start()

    serve_base = jnp.where(me == 0, turn_of_first, me)

    def serve_next(steps):
        pl.when(serve_base + steps < count)(lambda: serve(serve_base + steps))

    def serve_rest(steps):
        @pl.loop(serve_base + steps, count)
        def _(to):
            serve(to)

        @pl.when(rank < turn_of_first)
        def _():
            serve(0)

    def prepare():
        serve_next(1)
        serve_next(2)
        copies[3].wait()
        gate = dot(tok_s[...], wb_s[...]).astype(bf16).astype(f32)
        gate_s[...] = gate
        edge_send[0] = gate[span - 1 : span, :]
        edge_send[1] = gate[0:1, :]

        for c in copies[4:]:
            c.wait()

        chan_s[...] = jnp.zeros_like(chan_s)
        chan_s[0:3, :] = taps_s[0].astype(f32)
        chan_s[8:11, :] = taps_s[1].astype(f32)
        chan_s[16:18, :] = fb_s[...]
        chan_s[24:25, :] = ld_s[...]
        cols_s[...] = pick(one_hot(count * own, share, me * own, own), chan_s[...])
        hid_eye = one_hot(hid, hid, 0, hid)
        feature_total = pw_s.shape[0]
        padded = feat_s.shape[0] // 2
        pw2_s[...] = jnp.zeros_like(pw2_s)
        pw2_s[0:feature_total, :] = pw_s[...]
        pw2_s[padded : padded + feature_total, :] = pw_s[...]
        np_s[...] = jnp.zeros_like(np_s)
        np_s[0:2, :] = sf_s[...]
        np_s[8:9, :] = pb_s[...]
        np_s[16:17, :] = hb_s[...]
        net = pick(hid_eye, np_s[...])
        scale_a = net[:, 0:1] * (0.5 / math.pi)
        scale_b = net[:, 1:2] * (0.5 / math.pi)
        shift_a = net[:, 8:9] * scale_a
        shift_b = net[:, 16:17] * scale_b
        first_high, first_low = split(pick(hid_eye, pw2_s[...]))
        first_low = first_low[:, :padded]

        def three(table):
            high, low = split(table)
            lane = lax.broadcasted_iota(jnp.int32, table.shape, 1)
            return jnp.where(lane < 2 * hid, high.astype(f32), low.astype(f32)).astype(bf16)

        hw = hw_s[...]
        second = three(pick(hid_eye, jnp.concatenate([hw, hw, hw], axis=0)))
        own_hot = one_hot(own, share, me * own, own)
        weights = []
        for order in range(2):
            for side in range(2):
                w = fo_s[:, order, side, :]
                weights.append(pick(own_hot, jnp.concatenate([w, w, w], axis=0)))
        third = three(jnp.concatenate(weights, axis=0))
        decay = cols_s[0:own, 24:25]

        serve_next(3)

        blocks = 4
        width = length // blocks

        @pl.loop(0, blocks)
        def _(block):
            base = pl.multiple_of(block * width, width)
            feats = feat_s[:, pl.ds(base, width)]
            pre = dot(first_high, feats) + dot(first_low, feats[:padded])
            hidden = sine_of_turns(pre * scale_a + shift_a, coefficients)
            high, low = split(hidden)
            pre = dot(second, jnp.concatenate([high, low, high], axis=0))
            hidden = sine_of_turns(pre * scale_b + shift_b, coefficients)
            high, low = split(hidden)
            raw = dot(third, jnp.concatenate([high, low, high], axis=0))
            position = base + lax.broadcasted_iota(jnp.int32, (own, width), 1)
            scaled = position.astype(f32) * (1.0 / max(length - 1, 1))
            envelope = jnp.exp(-scaled * decay) + WINDOW_SHIFT
            later = jnp.where(position == 0, 0.0, envelope)
            for order in range(2):
                ahead = raw[2 * order * own : (2 * order + 1) * own] * envelope
                behind = raw[(2 * order + 1) * own : (2 * order + 2) * own] * later
                for kind, both in enumerate((ahead + behind, ahead - behind)):
                    high, low = split(both)
                    for part in range(width // span):
                        row = pl.multiple_of(block * (width // span) * own + part * own, own)
                        lanes = slice(part * span, (part + 1) * span)
                        kin_s[order, kind, 0, pl.ds(row, own), :] = high[:, lanes]
                        kin_s[order, kind, 1, pl.ds(row, own), :] = low[:, lanes]

            @pl.when(lax.rem(block, 2) == 1)
            def _():
                serve_next(4 + lax.div(block, 2))

        for part, target in enumerate((tr_s, ti_s)):
            one = turn_s[part * count : (part + 1) * count, :]
            target[...] = jnp.broadcast_to(one[:, None, :], (count, own, span)).reshape(rows, span)

        for order in range(2):
            sr, si = outer((kin_s[order, 0, 0], kin_s[order, 0, 1]), True, split)
            spec_s[order, 0] = (by_real(sr, True) + by_imag(minus(si), True)) * (1.0 / length)
            dr, di = outer((kin_s[order, 1, 0], kin_s[order, 1, 1]), True, split)
            spec_s[order, 1] = (by_imag(dr, True) + by_real(di, True)) * (1.0 / length)
            if order == 0:
                serve_rest(6)

    def short(ref, first):
        p = ref[...].astype(f32)
        lane = lax.broadcasted_iota(jnp.int32, (rows, span), 1)
        none = jnp.zeros((own, span), f32)
        back = pltpu.roll(p, 1, 1)
        back = jnp.where(lane == 0, jnp.concatenate([none, back[:-own]], axis=0), back)
        ahead = pltpu.roll(p, span - 1, 1)
        ahead = jnp.where(lane == span - 1, jnp.concatenate([ahead[own:], none], axis=0), ahead)
        tap = [cols_s[:, first + i : first + i + 1] for i in range(3)]
        return (back * tap[0] + p * tap[1] + ahead * tap[2]).astype(bf16)

    def one(values):
        return (values.astype(bf16),)

    def convolve(order, values, signal):
        hr, hi = outer(values, False, one)
        xr = by_real(hr) + by_imag(minus(hi))
        xi = by_imag(hr) + by_real(hi)
        kr, ki = spec_s[order, 0], spec_s[order, 1]
        yr = one(xr * kr - xi * ki)
        yi = one(xr * ki + xi * kr)
        ur = by_real(yr) + by_imag(yi)
        ui = by_real(yi) + by_imag(minus(yr))
        tr, ti = tr_s[...], ti_s[...]
        wr = split(ur * tr + ui * ti)
        wi = split(ui * tr - ur * ti)
        y = signal * cols_s[:, 16 + order : 17 + order]
        for part in wr:
            y = y + dot(bwd_s[0:rows, 0:rows], part)
        for part in wi:
            y = y + dot(bwd_s[0:rows, rows : 2 * rows], part)
        return y

    prepare()

    @pl.when(has_above)
    def _():
        edge(0).start()

    @pl.when(has_below)
    def _():
        edge(1).start()

    to_all(lambda to: remote(0, to, send_v, recv_v).wait_recv())
    value = short(recv_v, 0)
    first_conv = convolve(0, (value,), value.astype(f32))
    to_all(lambda to: remote(1, to, send_a, recv_a).wait_recv())
    gated = short(recv_a, 8).astype(f32) * first_conv
    send_o[...] = convolve(1, split(gated), gated).astype(bf16)

    @pl.loop(0, count)
    def _(to):
        @pl.when(to != me)
        def _():
            remote(2, to, send_o, recv_o).start()

    recv_o[mine, :] = send_o[mine, :]

    @pl.when(has_above)
    def _():
        edge(0).wait_send()
        edge(1).wait_recv()

    @pl.when(has_below)
    def _():
        edge(1).wait_send()
        edge(0).wait_recv()

    gate = gate_s[...]
    row = lax.broadcasted_iota(jnp.int32, (span, share), 0)
    above = jnp.where(me == 0, 0.0, edge_recv[0])
    below = jnp.where(me == count - 1, 0.0, edge_recv[1])
    back = jnp.where(row == 0, above, pltpu.roll(gate, 1, 0))
    ahead = jnp.where(row == span - 1, below, pltpu.roll(gate, span - 1, 0))
    tap = taps_s[2].astype(f32)
    gate = (back * tap[0:1] + gate * tap[1:2] + ahead * tap[2:3]).astype(bf16).astype(f32)
    to_all(lambda to: remote(0, to, send_v, recv_v).wait_send())
    to_all(lambda to: remote(1, to, send_a, recv_a).wait_send())
    to_all(lambda to: remote(2, to, send_o, recv_o).wait_send())
    to_all(lambda to: remote(2, to, send_o, recv_o).wait_recv())
    out[...] = (gate * recv_o[...].astype(f32).T).astype(bf16)


def per_device(
    tokens,
    w_value,
    w_gate_a,
    w_gate_b,
    short_taps,
    pos_weight,
    pos_bias,
    sine_freq,
    hid_weight,
    hid_bias,
    filter_out,
    filter_bias,
    lag_decay,
):
    count = lax.axis_size("row")
    span, depth = tokens.shape
    share = w_value.shape[1]
    own = share // count
    rows = count * own
    hid = hid_weight.shape[0]
    feature_total = pos_weight.shape[0]
    forward, backward, turns, features = make_constants(count, own, span, feature_total)
    operands = [
        tokens,
        w_value,
        w_gate_a,
        w_gate_b,
        short_taps,
        pos_weight,
        pos_bias[None, :],
        sine_freq,
        hid_weight,
        hid_bias[None, :],
        filter_out,
        filter_bias,
        lag_decay[None, :],
        jnp.asarray(features),
        jnp.asarray(forward),
        jnp.asarray(backward),
        jnp.asarray(turns),
    ]
    cut = {4: (3, 3, share), 11: (2, share), 12: (1, share)}
    landing = [pltpu.VMEM(cut.get(i, x.shape), x.dtype) for i, x in enumerate(operands)]
    square = pltpu.VMEM((rows, span), bf16)
    scratch = [
        *landing,
        pltpu.VMEM((features.shape[0], hid), f32),
        pltpu.VMEM((24, hid), f32),
        pltpu.VMEM((32, share), f32),
        square,
        square,
        square,
        square,
        square,
        square,
        pltpu.VMEM((2, 1, share), f32),
        pltpu.VMEM((2, 1, share), f32),
        pltpu.VMEM((span, share), f32),
        pltpu.VMEM((rows, 32), f32),
        pltpu.VMEM((2, 2, 2, rows, span), bf16),
        pltpu.VMEM((2, 2, rows, span), f32),
        pltpu.VMEM((rows, span), f32),
        pltpu.VMEM((rows, span), f32),
        pltpu.SemaphoreType.REGULAR((count,)),
        pltpu.SemaphoreType.DMA((len(operands),)),
        pltpu.SemaphoreType.DMA((4, count)),
        pltpu.SemaphoreType.DMA((4, count)),
    ]
    return pl.pallas_call(
        functools.partial(kernel, count, own, hid, sine_coefficients()),
        out_shape=pltpu.VMEM((span, share), bf16),
        in_specs=[pl.BlockSpec(memory_space=pl.ANY)] * len(operands),
        out_specs=pl.BlockSpec(memory_space=pltpu.VMEM),
        scratch_shapes=scratch,
        compiler_params=pltpu.CompilerParams(collective_id=0, has_side_effects=True),
        name="gated_conv",
    )(*operands)


def solution(mesh):
    in_specs = (
        P(("grp", "row"), None),
        P(None, "col"),
        P(None, "col"),
        P(None, "col"),
        P(),
        P(),
        P(),
        P(),
        P(),
        P(),
        P(None, None, None, "col"),
        P(),
        P(),
    )
    out_specs = P(("grp", "row"), "col")
    return jax.shard_map(
        per_device, mesh=mesh, in_specs=in_specs, out_specs=out_specs, check_vma=False
    )
```
